256 devices in a mesh: sp: 32 (over z, x), tp: 8 (over y, core).
Axes of the slice: x: 4, y: 4, z: 8, core: 2. Of those that a mesh axis runs over, the one named last changes fastest.
Arguments:
- residual_matrix: bfloat16 [8192, 2048], P(('sp', 'tp')), may hold values from -6 to 6
- query_vectors: bfloat16 [2048, 8192], P('tp', 'sp'), may hold values from -6 to 6
- lookup_vectors: bfloat16 [2048, 8192], P('tp', 'sp'), may hold values from -6 to 6
- payload_vectors: bfloat16 [2048, 8192], P('tp', 'sp'), may hold values from -6 to 6
- fading_dependent_term: bfloat16 [2048, 8192], P('tp', 'sp'), may hold values from -4 to 4
- step_size_preactivation: bfloat16 [2048, 8192], P('tp', 'sp'), may hold values from -8 to 8
- attention_result_switch: bfloat16 [2048, 8192], P('tp', 'sp'), may hold values from -6 to 6
- fading_bias_vector: float32 [2048], P('tp'), may hold values from -16 to -2
- surplus_forgetting: float32 [32, 8192], P('tp', 'sp'), may hold values from -0.7 to 0
- per_group_scaler: float32 [2048], P('tp'), may hold values from 0.1 to 1.9
- attention_result_matrix: bfloat16 [2048, 2048], P('tp'), may hold values from -0.125 to 0.125
- dense_block_scaler: float32 [2048], replicated, may hold values from 0.1 to 1.9
- switching_matrix: bfloat16 [2048, 5632], P('sp', 'tp'), may hold values from -0.125 to 0.125
- expanding_matrix: bfloat16 [2048, 5632], P('sp', 'tp'), may hold values from -0.125 to 0.125
- contracting_matrix: bfloat16 [5632, 2048], P('tp', 'sp'), may hold values from -0.078125 to 0.078125
Outputs:
- blended: bfloat16 [8192, 2048], P(('sp', 'tp'))
The draws below stay inside these ranges and needn't reach their ends.
All inputs are finite; a program needn't handle non-finite values.
Results may differ from the reference program's by a relative error of at most 0.015.
Values may be sent and summed in bfloat16 or wider, within the bound.
No kernel may reach another device: no remote copies, remote signals or barrier semaphores. Data moves between devices by JAX's collectives and lax.ppermute only.
A program may use at most 128 MiB of HBM per device.

```python
import math
import jax
import jax.numpy as jnp
from jax import lax

D = 2048
HEAD = 64
HEADS = 32
FF = 5632
BLOCK = 64
TOK_DEV = 256
MIX = 2048
TOKENS = 8192
N_TP = 8


def draw_lookup_vectors(key, part):
    noise_key = jax.random.fold_in(key, 41)
    quiet_key = jax.random.fold_in(key, 42)
    level_key = jax.random.fold_in(key, 43)
    direction_key = jax.random.fold_in(key, 44)
    block_key = jax.random.fold_in(key, 45)
    noise = jnp.clip(jax.random.normal(noise_key, (HEADS, HEAD, TOKENS), jnp.float32), -5.0, 5.0)
    quiet = jax.random.uniform(quiet_key, (HEADS, HEAD, 1), jnp.float32) < 0.25
    quiet_level = jnp.exp(jax.random.uniform(level_key, (HEADS, HEAD, 1), jnp.float32, math.log(0.01), math.log(0.05)))
    position = jnp.arange(TOKENS)[None, None, :]
    later = position >= TOK_DEV
    factor = jnp.where(jnp.logical_and(quiet, later), quiet_level, 1.0)
    direction = jax.random.normal(direction_key, (HEADS, HEAD, 1), jnp.float32)
    direction = direction * (3.0 / jnp.sqrt(jnp.sum(direction * direction, axis=1, keepdims=True) + 1e-06))
    chosen = jax.random.uniform(block_key, (HEADS, 1, TOKENS // BLOCK), jnp.float32) < 0.25
    chosen = jnp.repeat(chosen, BLOCK, axis=2)
    keys = (noise + jnp.where(chosen, direction, 0.0)) * factor
    return jnp.clip(keys, -6.0, 6.0).reshape(MIX, TOKENS).astype(jnp.bfloat16)


def draw_fading_bias_vector(key, part):
    first_key = jax.random.fold_in(key, 11)
    second_key = jax.random.fold_in(key, 12)
    fast_share = 0.5
    fast_heads = jax.random.uniform(first_key, (HEADS, 1), jnp.float32) < fast_share
    jitter = jax.random.uniform(second_key, (HEADS, HEAD), jnp.float32, -0.5, 0.5)
    slow_level = math.log(0.6 / TOKENS) + 0.5
    return (jnp.where(fast_heads, -3.4, slow_level) + jitter).reshape(HEADS * HEAD).astype(jnp.float32)


def draw_fading_dependent_term(key, part):
    first_key = jax.random.fold_in(key, 21)
    second_key = jax.random.fold_in(key, 22)
    noise = jnp.clip(jax.random.normal(first_key, (MIX, TOKENS), jnp.float32) * 0.7, -3.0, 3.0)
    levels = jax.random.uniform(second_key, (TOKENS // TOK_DEV,), jnp.float32, -0.7, 0.7)
    return (noise + jnp.repeat(levels, TOK_DEV)[None, :]).astype(jnp.bfloat16)


def draw_surplus_forgetting(key, part):
    first_key = jax.random.fold_in(key, 31)
    second_key = jax.random.fold_in(key, 32)
    struck = jax.random.uniform(first_key, (HEADS, TOKENS), jnp.float32) < 3.0 / TOKENS
    losses = jnp.log(jax.random.uniform(second_key, (HEADS, TOKENS), jnp.float32, 0.5, 0.8))
    return jnp.where(struck, losses, 0.0).astype(jnp.float32)


def shard_levels(own_key, extent, shards, smallest, high):
    factor_of = 1.0
    for dim, shards_of in shards:
        heights = jax.random.uniform(jax.random.fold_in(jax.random.fold_in(own_key, 6), dim), (shards_of,), jnp.float32, smallest / len(shards), high / len(shards))
        factor_of = factor_of * jnp.repeat(jnp.exp(heights), extent[dim] // shards_of).reshape((-1,) + (1,) * (len(extent) - 1 - dim))
    return factor_of


def bell_draw(key, extent, spread, limit, split=(), kind=jnp.bfloat16):
    entries = spread * jax.random.normal(key, extent, jnp.float32)
    if split:
        entries = entries * shard_levels(key, extent, split, -0.22, 0.18)
    return jnp.clip(entries, -limit, limit).astype(kind)


def setup_inputs(seed: int = 0) -> dict:
    streams_of = jax.random.split(jax.random.key(seed), 16)
    residual_matrix = bell_draw(streams_of[0], (TOKENS, D), 1.0, 6.0, ((0, 256),))
    query_vectors = bell_draw(streams_of[1], (MIX, TOKENS), 1.0, 6.0, ((0, 8), (1, 32)))
    lookup_vectors = draw_lookup_vectors(jax.random.fold_in(streams_of[15], 71), 0)
    payload_vectors = bell_draw(streams_of[3], (MIX, TOKENS), 1.0, 6.0, ((0, 8), (1, 32)))
    fading_dependent_term = draw_fading_dependent_term(jax.random.fold_in(streams_of[15], 71), 0)
    step_size_preactivation = bell_draw(streams_of[5], (MIX, TOKENS), 1.5, 8.0, ((0, 8), (1, 32)))
    attention_result_switch = bell_draw(streams_of[6], (MIX, TOKENS), 1.0, 6.0, ((0, 8), (1, 32)))
    fading_bias_vector = draw_fading_bias_vector(jax.random.fold_in(streams_of[15], 71), 0)
    surplus_forgetting = draw_surplus_forgetting(jax.random.fold_in(streams_of[15], 71), 0)
    per_group_scaler = jnp.clip(1.0 + 0.18 * jax.random.normal(streams_of[9], (MIX,), jnp.float32), 0.1, 1.9)
    attention_result_matrix = bell_draw(streams_of[10], (MIX, D), MIX ** -0.5, 0.125, ((0, 8),))
    dense_block_scaler = jnp.clip(1.0 + 0.18 * jax.random.normal(streams_of[11], (D,), jnp.float32), 0.1, 1.9)
    switching_matrix = bell_draw(streams_of[12], (D, FF), D ** -0.5, 0.125, ((0, 32), (1, 8)))
    expanding_matrix = bell_draw(streams_of[13], (D, FF), D ** -0.5, 0.125, ((0, 32), (1, 8)))
    contracting_matrix = bell_draw(streams_of[14], (FF, D), FF ** -0.5, 0.078125, ((0, 8), (1, 32)))
    return dict(residual_matrix=residual_matrix, query_vectors=query_vectors, lookup_vectors=lookup_vectors, payload_vectors=payload_vectors, fading_dependent_term=fading_dependent_term, step_size_preactivation=step_size_preactivation, attention_result_switch=attention_result_switch, fading_bias_vector=fading_bias_vector, surplus_forgetting=surplus_forgetting, per_group_scaler=per_group_scaler, attention_result_matrix=attention_result_matrix, dense_block_scaler=dense_block_scaler, switching_matrix=switching_matrix, expanding_matrix=expanding_matrix, contracting_matrix=contracting_matrix)


norm_eps = 1e-06
group_eps = 0.00064
key_eps = 1e-06
highest = lax.Precision.HIGHEST

def per_token(source):
    return source.astype(jnp.float32).reshape(HEADS, HEAD, TOKENS).transpose(2, 0, 1)

def reference(residual_matrix, query_vectors, lookup_vectors, payload_vectors, fading_dependent_term, step_size_preactivation, attention_result_switch, fading_bias_vector, surplus_forgetting, per_group_scaler, attention_result_matrix, dense_block_scaler, switching_matrix, expanding_matrix, contracting_matrix):
    read_rows = per_token(query_vectors)
    key_rows = per_token(lookup_vectors)
    value_rows = per_token(payload_vectors)
    fading_preactivation = per_token(fading_dependent_term) + fading_bias_vector.reshape(HEADS, HEAD)[None]
    log_fading_factor = -jnp.exp(-jax.nn.softplus(-fading_preactivation) - 0.5) + surplus_forgetting.T[:, :, None]
    learn_rate = jax.nn.sigmoid(per_token(step_size_preactivation))
    unit_keys = key_rows * lax.rsqrt(lax.optimization_barrier(jnp.sum(key_rows * key_rows, axis=-1, keepdims=True)) + key_eps)
    scaled = key_rows * learn_rate
    removal = unit_keys * learn_rate

    def advance(carried, member):
        read_step, decay_step, unit_step, removal_step, key_step, value_step = member
        seen_part = jnp.einsum('hij,hj->hi', carried, unit_step, precision=highest)
        carried = carried * decay_step[:, None, :] - seen_part[:, :, None] * removal_step[:, None, :] + value_step[:, :, None] * key_step[:, None, :]
        return (carried, jnp.einsum('hij,hj->hi', carried, read_step, precision=highest))
    zero_state = jnp.zeros((HEADS, HEAD, HEAD), jnp.float32)
    _, outputs = lax.scan(advance, zero_state, (read_rows, jnp.exp(log_fading_factor), unit_keys, removal, scaled, value_rows))
    centred = outputs - lax.optimization_barrier(jnp.mean(outputs, axis=-1, keepdims=True))
    variance = lax.optimization_barrier(jnp.mean(centred * centred, axis=-1, keepdims=True))
    normed_heads = (centred * lax.rsqrt(variance + group_eps)).reshape(TOKENS, HEADS * HEAD)
    mixed_out = (normed_heads * per_group_scaler[None, :] * attention_result_switch.astype(jnp.float32).T).astype(jnp.bfloat16)
    middle = residual_matrix.astype(jnp.float32) + jnp.dot(mixed_out, attention_result_matrix, preferred_element_type=jnp.float32)
    normed = (middle * lax.rsqrt(lax.optimization_barrier(jnp.mean(middle * middle, axis=-1, keepdims=True)) + norm_eps) * dense_block_scaler).astype(jnp.bfloat16)
    gate_sum = jnp.dot(normed, switching_matrix, preferred_element_type=jnp.float32)
    up_sum = jnp.dot(normed, expanding_matrix, preferred_element_type=jnp.float32)
    hidden = (jax.nn.silu(gate_sum) * up_sum).astype(jnp.bfloat16)
    group_width = FF // N_TP

    def add_group(total_sum, group_index):
        piece_rows = lax.dynamic_slice_in_dim(hidden, group_index * group_width, group_width, 1)
        down_rows = lax.dynamic_slice_in_dim(contracting_matrix, group_index * group_width, group_width, 0)
        product = jnp.dot(piece_rows, down_rows, preferred_element_type=jnp.float32)
        rounded = lax.optimization_barrier(product.astype(jnp.bfloat16))
        return (total_sum + rounded.astype(jnp.float32), None)
    channel_out, _ = lax.scan(add_group, jnp.zeros((TOKENS, D), jnp.float32), jnp.arange(N_TP, dtype=jnp.int32))
    return (middle + channel_out).astype(jnp.bfloat16)
```

```python
import functools

import jax
import jax.numpy as jnp
from jax import lax
from jax.experimental import pallas as pl
from jax.experimental.pallas import tpu as pltpu
from jax.sharding import Mesh
from jax.sharding import PartitionSpec as P

HEAD = 64
BLOCK = 64
GROUPS = 4
SPAN = 256
BLOCKS = SPAN // BLOCK
SP = ("z", "x")
TP = ("y", "c")
ALL = ("z", "x", "y", "c")

norm_eps = 1e-06
group_eps = 0.00064
key_eps = 1e-06
half_power = 0.6065306597126334

f32 = jnp.float32
bf16 = jnp.bfloat16


def pair(a):
    if a.dtype == bf16:
        return (a,)
    high = a.astype(bf16)
    return (high, (a - high.astype(f32)).astype(bf16))


def mm(a, b, dims=((1,), (0,))):
    a = a if isinstance(a, tuple) else pair(a)
    b = b if isinstance(b, tuple) else pair(b)
    dot = lambda l, r: lax.dot_general(l, r, (dims, ((), ())), preferred_element_type=f32)
    total = dot(a[0], b[0])
    if len(b) > 1:
        total = total + dot(a[0], b[1])
    if len(a) > 1:
        total = total + dot(a[1], b[0])
    return total


def sigmoid(x):
    return 1.0 / (1.0 + jnp.exp(-x))


def down_rows(row, width):
    turned = jnp.broadcast_to(row, (128, row.shape[1])).T
    return jnp.concatenate([turned] * (width // 128), axis=1)


def square_iotas():
    return (
        lax.broadcasted_iota(jnp.int32, (SPAN, SPAN), 0),
        lax.broadcasted_iota(jnp.int32, (SPAN, SPAN), 1),
    )


def head_rows(h):
    return slice(h * HEAD, (h + 1) * HEAD)


def local_kernel(
    key_ref, value_ref, query_ref, fading_ref, rate_ref, bias_ref, surplus_ref,
    pack_ref, prefix_ref, basis_ref, offset_ref, removal_ref, scaled_ref, reads_ref,
):
    row, col = square_iotas()
    same = (row // BLOCK) == (col // BLOCK)
    fading = fading_ref[...].astype(f32) + down_rows(bias_ref[...], SPAN)
    surplus = jnp.concatenate(
        [jnp.broadcast_to(surplus_ref[h : h + 1, :], (HEAD, SPAN)) for h in range(GROUPS)], axis=0
    )
    log_decay = surplus - half_power * sigmoid(fading)
    rate = sigmoid(rate_ref[...].astype(f32))
    keys = key_ref[...].astype(f32)
    norms = jnp.concatenate(
        [
            jnp.broadcast_to(
                lax.rsqrt(
                    jnp.sum(keys[head_rows(h)] * keys[head_rows(h)], axis=0, keepdims=True) + key_eps
                ),
                (HEAD, SPAN),
            )
            for h in range(GROUPS)
        ],
        axis=0,
    )
    unit = keys * norms
    scaled = keys * rate
    removal = unit * rate
    first = log_decay.astype(bf16)
    rest = log_decay - first.astype(f32)
    second = rest.astype(bf16)
    third = (rest - second.astype(f32)).astype(bf16)
    upto = jnp.where(same & (row <= col), 1.0, 0.0).astype(bf16)
    every = jnp.where(same, 1.0, 0.0).astype(bf16)
    running = lambda m: mm((first,), (m,)) + mm((second,), (m,)) + mm((third,), (m,))
    after = running(upto)
    final = running(every)
    probe = unit * jnp.exp(after - log_decay)
    grow = jnp.exp(-after)
    removal_in = removal * grow
    scaled_in = scaled * grow
    end = jnp.exp(final - after)
    removal_end = removal * end
    scaled_end = scaled * end
    block_decay = jnp.exp(final)
    reads_ref[...] = query_ref[...].astype(f32) * jnp.exp(after)
    strict = same & (row < col)
    in16 = (row // 16) == (col // 16)
    in32 = (row // 32) == (col // 32)
    eye = (row == col).astype(f32)
    eye_head = eye[:HEAD, :HEAD]
    lane = lax.broadcasted_iota(jnp.int32, (HEAD, SPAN), 1) // BLOCK
    for h in range(GROUPS):
        rows = head_rows(h)
        probe_h = pair(probe[rows])
        removal_t = removal_in[rows].T
        scaled_t = scaled_in[rows].T
        removal_ref[h] = removal_t
        scaled_ref[h] = scaled_t
        mutual = jnp.where(strict, mm(removal_t, probe_h), 0.0)
        through = jnp.where(strict, mm(scaled_t, probe_h), 0.0)
        value = value_ref[rows, :]
        near = jnp.where(in16, mutual, 0.0)
        power = pair(-near)
        inverse = eye - near
        for level in range(3):
            square = mm(power, power)
            power = pair(square)
            inverse = inverse + mm(inverse, power)
        for inner, outer in ((in16, in32), (in32, same)):
            link = pair(jnp.where(outer & ~inner, mutual, 0.0))
            parts = pair(inverse)
            inverse = inverse - mm(mm(parts, link), parts)
        parts = pair(inverse)
        basis = mm(probe_h, parts)
        offset = mm(mm(value, through), parts)
        basis_ref[rows, :] = basis
        offset_ref[rows, :] = offset
        stacked = jnp.concatenate(
            [jnp.where(lane == b, basis, 0.0) for b in range(BLOCKS)]
            + [jnp.where(lane == b, offset, 0.0) for b in range(BLOCKS)],
            axis=0,
        )
        taken = mm(stacked, removal_end[rows].T)
        value_f = value.astype(f32)
        given = mm(
            jnp.concatenate([jnp.where(lane == b, value_f, 0.0) for b in range(BLOCKS)], axis=0).astype(bf16),
            scaled_end[rows].T,
        )
        decay_h = block_decay[rows]
        total = None
        for b in range(BLOCKS):
            at = slice(b * HEAD, (b + 1) * HEAD)
            over = slice((BLOCKS + b) * HEAD, (BLOCKS + b + 1) * HEAD)
            carry_map = eye_head * decay_h[:, b * BLOCK : b * BLOCK + 1] - taken[at]
            carry_add = given[at] - taken[over]
            if total is None:
                total = jnp.concatenate([carry_map, carry_add], axis=0)
            else:
                prefix_ref[h, b - 1] = total
                total = mm(total, carry_map)
                total = jnp.concatenate([total[:HEAD], total[HEAD:] + carry_add], axis=0)
        pack_ref[rows, :] = jnp.concatenate([total[:HEAD], total[HEAD:]], axis=1).astype(bf16)


def reach_kernel(
    prefix_ref, basis_ref, offset_ref, removal_ref, scaled_ref, reads_ref, value_ref, state_ref, own_ref
):
    row, col = square_iotas()
    upto = ((row // BLOCK) == (col // BLOCK)) & (row <= col)
    lane = lax.broadcasted_iota(jnp.int32, (HEAD, SPAN), 1) // BLOCK
    for h in range(GROUPS):
        rows = head_rows(h)
        reads = reads_ref[rows, :]
        reads_p = pair(reads)
        reach_removal = pair(jnp.where(upto, mm(removal_ref[h], reads_p), 0.0))
        reach_value = jnp.where(upto, mm(scaled_ref[h], reads_p), 0.0)
        effect = reads - mm(basis_ref[rows, :], reach_removal)
        own = mm(value_ref[rows, :], reach_value) - mm(offset_ref[rows, :], reach_removal)
        state = jnp.where(lane == 0, effect, 0.0)
        for b in range(1, BLOCKS):
            both = mm(prefix_ref[h, b - 1], jnp.where(lane == b, effect, 0.0))
            state = state + both[:HEAD]
            own = own + both[HEAD:]
        state_ref[rows, :] = state
        own_ref[rows, :] = own


def after_pack(total, pack):
    moved = mm(total, pack[:, :HEAD])
    return jnp.concatenate(
        [moved[:HEAD], moved[HEAD:] + pack[:, HEAD:].astype(f32)], axis=0
    )


def row_kernel(index_ref, own_ref, one_ref, two_ref, three_ref, pack_ref, before_ref, held):
    mine = index_ref[1]
    for shift, ref in enumerate((own_ref, one_ref, two_ref, three_ref)):
        held[(mine + 4 - shift) % 4] = ref[...]
    eye = (
        lax.broadcasted_iota(jnp.int32, (HEAD, HEAD), 0)
        == lax.broadcasted_iota(jnp.int32, (HEAD, HEAD), 1)
    ).astype(f32)
    start = jnp.concatenate([eye, jnp.zeros((HEAD, HEAD), f32)], axis=0)
    for h in range(GROUPS):
        rows = head_rows(h)
        members = [held[k, rows, :] for k in range(4)]
        first = jnp.concatenate(
            [members[0][:, :HEAD], members[0][:, HEAD:]], axis=0
        ).astype(f32)
        second = after_pack(first, members[1])
        third = after_pack(second, members[2])
        fourth = after_pack(third, members[3])
        before = jnp.where(
            mine == 0, start, jnp.where(mine == 1, first, jnp.where(mine == 2, second, third))
        )
        before_ref[h] = before
        pack_ref[rows, :] = jnp.concatenate([fourth[:HEAD], fourth[HEAD:]], axis=1).astype(bf16)


def mixed_kernel(
    index_ref, planes_ref, before_ref, state_ref, own_ref, switch_ref, scaler_ref, keep_ref, send_ref, held
):
    plane = index_ref[0]
    y = index_ref[2]
    core = index_ref[3]
    carried = [jnp.zeros((HEAD, HEAD), f32) for _ in range(GROUPS)]
    for k in range(7):
        passed = k < plane
        for h in range(GROUPS):
            member = planes_ref[k, head_rows(h), :]
            moved = mm(carried[h], member[:, :HEAD]) + member[:, HEAD:].astype(f32)
            carried[h] = jnp.where(passed, moved, carried[h])
    heads = []
    for h in range(GROUPS):
        rows = head_rows(h)
        entering = mm(carried[h], before_ref[h, :HEAD]) + before_ref[h, HEAD:]
        outputs = mm(entering, state_ref[rows, :]) + own_ref[rows, :]
        centred = outputs - jnp.mean(outputs, axis=0, keepdims=True)
        heads.append(
            centred * lax.rsqrt(jnp.mean(centred * centred, axis=0, keepdims=True) + group_eps)
        )
    mixed = jnp.concatenate(heads, axis=0) * down_rows(scaler_ref[...], SPAN)
    mixed = mixed * switch_ref[...].astype(f32)
    held[...] = mixed.T.astype(bf16).reshape(8, 32, SPAN)
    for s in range(4):
        at = 2 * ((y + s) % 4)
        keep_ref[s] = held[at + core]
        send_ref[s] = held[at + 1 - core]


def project_kernel(keep_ref, got_ref, own_ref, other_ref, here_ref, one_ref, two_ref, three_ref):
    dot = functools.partial(jnp.dot, preferred_element_type=f32)
    rows = dot(keep_ref[...].reshape(128, SPAN), own_ref[...])
    rows = rows + dot(got_ref[...].reshape(128, SPAN), other_ref[...])
    here_ref[...] = rows[:32]
    one_ref[...] = rows[32:64].astype(bf16)
    two_ref[...] = rows[64:96].astype(bf16)
    three_ref[...] = rows[96:].astype(bf16)


VMEM = pl.BlockSpec(memory_space=pltpu.VMEM)
SMEM = pl.BlockSpec(memory_space=pltpu.SMEM)


def like(shape, kind=f32):
    return jax.ShapeDtypeStruct(shape, kind)


def whole(kernel, outs, *args, scratch=(), scalars=0, flops=0, name=None):
    specs = [SMEM] * scalars + [VMEM] * (len(args) - scalars)
    return pl.pallas_call(
        kernel,
        out_shape=outs,
        in_specs=specs,
        out_specs=jax.tree.map(lambda _: VMEM, outs),
        scratch_shapes=scratch,
        cost_estimate=pl.CostEstimate(flops=flops, transcendentals=0, bytes_accessed=1 << 20),
        name=name,
    )(*args)


def moved(x, axis, shift):
    size = lax.axis_size(axis)
    return lax.ppermute(x, axis, [(k, (k + shift) % size) for k in range(size)])


def rms_rows(middle, dense_block_scaler):
    scale_rows = lax.rsqrt(jnp.mean(middle * middle, axis=-1, keepdims=True) + norm_eps)
    return (middle * scale_rows * dense_block_scaler).astype(bf16)


def hidden_of(normed, gate_full, up_full):
    gate_sum = jnp.dot(normed, gate_full, preferred_element_type=f32)
    up_sum = jnp.dot(normed, up_full, preferred_element_type=f32)
    return (jax.nn.silu(gate_sum) * up_sum).astype(bf16)


def gathered_weights(switching_matrix, expanding_matrix, contracting_matrix):
    both = jnp.concatenate([switching_matrix, expanding_matrix, contracting_matrix.T], axis=1)
    full = lax.all_gather(both, SP, axis=0, tiled=True)
    width = switching_matrix.shape[1]
    return full[:, :width], full[:, width : 2 * width], full[:, 2 * width :]


def local(
    residual_matrix,
    query_vectors,
    lookup_vectors,
    payload_vectors,
    fading_dependent_term,
    step_size_preactivation,
    attention_result_switch,
    fading_bias_vector,
    surplus_forgetting,
    per_group_scaler,
    attention_result_matrix,
    dense_block_scaler,
    switching_matrix,
    expanding_matrix,
    contracting_matrix,
):
    index = jnp.stack([lax.axis_index(a) for a in ALL]).astype(jnp.int32)
    gate_full, up_full, down_full = gathered_weights(
        switching_matrix, expanding_matrix, contracting_matrix
    )
    other_matrix = moved(attention_result_matrix, "c", 1)
    full = like((SPAN, SPAN))
    turned = like((GROUPS, SPAN, HEAD))
    pack, prefix, basis, offset, removal_t, scaled_t, reads = whole(
        local_kernel,
        (like((SPAN, 128), bf16), like((GROUPS, BLOCKS - 1, 128, HEAD)), full, full, turned, turned, full),
        lookup_vectors,
        payload_vectors,
        query_vectors,
        fading_dependent_term,
        step_size_preactivation,
        fading_bias_vector.reshape(1, -1),
        surplus_forgetting,
        flops=1 << 33,
        name="local",
    )
    others = [moved(pack, "x", s) for s in (1, 2, 3)]
    state, own = whole(
        reach_kernel, (full, full), prefix, basis, offset, removal_t, scaled_t, reads, payload_vectors,
        flops=1 << 32, name="reach",
    )
    row_pack, before = whole(
        row_kernel,
        (like((SPAN, 128), bf16), like((GROUPS, 128, HEAD))),
        index, pack, *others,
        scratch=[pltpu.VMEM((4, SPAN, 128), bf16)],
        scalars=1, flops=1 << 30, name="row",
    )
    planes = lax.all_gather(row_pack, "z")
    keep, send = whole(
        mixed_kernel,
        (like((4, 32, SPAN), bf16), like((4, 32, SPAN), bf16)),
        index, planes, before, state, own, attention_result_switch, per_group_scaler.reshape(1, -1),
        scratch=[pltpu.VMEM((8, 32, SPAN), bf16)],
        scalars=1, flops=1 << 30, name="mixed",
    )
    got = moved(send, "c", 1)
    here, *away = whole(
        project_kernel,
        (like((32, 2048)),) + (like((32, 2048), bf16),) * 3,
        keep, got, attention_result_matrix, other_matrix,
        flops=1 << 29, name="project",
    )
    middle = residual_matrix.astype(f32) + here
    for s, piece in enumerate(away, 1):
        middle = middle + moved(piece, "y", s).astype(f32)
    normed = rms_rows(middle, dense_block_scaler)
    mine = [normed] + [moved(normed, "y", s) for s in (1, 2, 3)]
    theirs = [moved(piece, "c", 1) for piece in mine]
    rows = jnp.concatenate(mine + theirs, axis=0)
    hidden = hidden_of(rows, gate_full, up_full)
    partial = lax.dot_general(
        hidden, down_full, (((1,), (1,)), ((), ())), preferred_element_type=f32
    ).astype(bf16)
    summed = partial[:128].astype(f32) + moved(partial[128:], "c", 1).astype(f32)
    channel_out = summed[:32]
    for s in (1, 2, 3):
        channel_out = channel_out + moved(
            summed[32 * s : 32 * s + 32].astype(bf16), "y", -s
        ).astype(f32)
    return (middle + channel_out).astype(bf16)


def solution(mesh):
    torus = Mesh(mesh.devices.reshape(8, 4, 4, 2), ALL)
    channels = P(TP, SP)
    placed = (
        P(ALL, None),
        channels,
        channels,
        channels,
        channels,
        channels,
        channels,
        P(TP),
        P(TP, SP),
        P(TP),
        P(TP, None),
        P(),
        P(SP, TP),
        P(SP, TP),
        P(TP, SP),
    )
    return jax.shard_map(
        local, mesh=torus, in_specs=placed, out_specs=P(ALL, None), check_vma=False
    )
```

```python
import functools

import jax
import jax.numpy as jnp
from jax import lax
from jax.experimental import pallas as pl
from jax.experimental.pallas import tpu as pltpu
from jax.sharding import Mesh
from jax.sharding import PartitionSpec as P

HEAD = 64
BLOCK = 64
GROUPS = 4
SPAN = 256
BLOCKS = SPAN // BLOCK
SP = ("z", "x")
TP = ("y", "c")
ALL = ("z", "x", "y", "c")

norm_eps = 1e-06
group_eps = 0.00064
key_eps = 1e-06
half_power = 0.6065306597126334

f32 = jnp.float32
bf16 = jnp.bfloat16


def pair(a):
    if a.dtype == bf16:
        return (a,)
    high = a.astype(bf16)
    return (high, (a - high.astype(f32)).astype(bf16))


def mm(a, b, dims=((1,), (0,))):
    a = a if isinstance(a, tuple) else pair(a)
    b = b if isinstance(b, tuple) else pair(b)
    dot = lambda l, r: lax.dot_general(l, r, (dims, ((), ())), preferred_element_type=f32)
    total = dot(a[0], b[0])
    if len(b) > 1:
        total = total + dot(a[0], b[1])
    if len(a) > 1:
        total = total + dot(a[1], b[0])
    return total


def sigmoid(x):
    return 1.0 / (1.0 + jnp.exp(-x))


def down_rows(row, width):
    turned = jnp.broadcast_to(row, (128, row.shape[1])).T
    return jnp.concatenate([turned] * (width // 128), axis=1)


def head_rows(h):
    return slice(h * HEAD, (h + 1) * HEAD)


def compressed_iotas():
    row = lax.broadcasted_iota(jnp.int32, (HEAD, SPAN), 0)
    lane = lax.broadcasted_iota(jnp.int32, (HEAD, SPAN), 1)
    return row, lane % BLOCK, lane // BLOCK


def same_block():
    row = lax.broadcasted_iota(jnp.int32, (SPAN, SPAN), 0) // BLOCK
    return jnp.where(row == lax.broadcasted_iota(jnp.int32, (SPAN, SPAN), 1) // BLOCK, 1.0, 0.0)


def spread(block, every):
    return jnp.concatenate([block] * BLOCKS, axis=0) * every


def by_block(left, right, every, turned=False):
    count = left.shape[0]
    dims = (((1,), (1,)) if turned else ((1,), (0,)), ((), ()))
    dot = lambda l, r: lax.dot_general(l, spread(r, every), dims, preferred_element_type=f32)
    left, right = pair(left), pair(right)
    if len(left) == 1:
        return dot(left[0], right[0]) + dot(left[0], right[1])
    both = dot(jnp.concatenate(left, axis=0), right[0])
    return both[:count] + both[count:] + dot(left[0], right[1])


def diagonal(full, block):
    total = jnp.where(block == 0, full[:HEAD], 0.0)
    for b in range(1, BLOCKS):
        total = total + jnp.where(block == b, full[b * HEAD : (b + 1) * HEAD], 0.0)
    return total


def reached(removal, scaled, seen, block):
    left = pair(jnp.concatenate([removal.T, scaled.T], axis=0))
    seen = pair(seen)
    dot = lambda l, r: jnp.dot(l, r, preferred_element_type=f32)
    both = dot(jnp.concatenate(left, axis=0), seen[0])
    both = both[: 2 * SPAN] + both[2 * SPAN :] + dot(left[0], seen[1])
    return diagonal(both[:SPAN], block), diagonal(both[SPAN:], block)


def local_kernel(
    key_ref, value_ref, query_ref, fading_ref, rate_ref, bias_ref, surplus_ref,
    pack_ref, prefix_ref, basis_ref, removal_ref, scaled_ref, reads_ref,
):
    every = same_block()
    row = lax.broadcasted_iota(jnp.int32, (SPAN, SPAN), 0)
    col = lax.broadcasted_iota(jnp.int32, (SPAN, SPAN), 1)
    upto = jnp.where(row <= col, every, 0.0).astype(bf16)
    every = every.astype(bf16)
    fading = fading_ref[...].astype(f32) + down_rows(bias_ref[...], SPAN)
    surplus = jnp.concatenate(
        [jnp.broadcast_to(surplus_ref[h : h + 1, :], (HEAD, SPAN)) for h in range(GROUPS)], axis=0
    )
    log_decay = surplus - half_power * sigmoid(fading)
    rate = sigmoid(rate_ref[...].astype(f32))
    keys = key_ref[...].astype(f32)
    norms = jnp.concatenate(
        [
            jnp.broadcast_to(
                lax.rsqrt(
                    jnp.sum(keys[head_rows(h)] * keys[head_rows(h)], axis=0, keepdims=True) + key_eps
                ),
                (HEAD, SPAN),
            )
            for h in range(GROUPS)
        ],
        axis=0,
    )
    unit = keys * norms
    scaled = keys * rate
    removal = unit * rate
    first = log_decay.astype(bf16)
    rest = log_decay - first.astype(f32)
    second = rest.astype(bf16)
    third = (rest - second.astype(f32)).astype(bf16)
    pieces = jnp.concatenate([first, second, third], axis=0)

    def running(m):
        sums = jnp.dot(pieces, m, preferred_element_type=f32)
        return sums[:SPAN] + sums[SPAN : 2 * SPAN] + sums[2 * SPAN :]

    after = running(upto)
    final = running(every)
    probe = unit * jnp.exp(after - log_decay)
    grow = jnp.exp(-after)
    removal_in = removal * grow
    scaled_in = scaled * grow
    end = jnp.exp(final - after)
    removal_end = removal * end
    scaled_end = scaled * end
    block_decay = jnp.exp(final)
    removal_ref[...] = removal_in
    scaled_ref[...] = scaled_in
    reads_ref[...] = query_ref[...].astype(f32) * jnp.exp(after)
    row, col, block = compressed_iotas()
    eye = (row == col).astype(f32)
    strict = row < col
    in16 = (row // 16) == (col // 16)
    in32 = (row // 32) == (col // 32)
    links = ((row // 16) != (col // 16)) & in32, ~in32
    for h in range(GROUPS):
        rows = head_rows(h)
        mutual, through = reached(removal_in[rows], scaled_in[rows], probe[rows], block)
        mutual = jnp.where(strict, mutual, 0.0)
        through = jnp.where(strict, through, 0.0)
        value = value_ref[rows, :]
        power = jnp.where(in16, -mutual, 0.0)
        inverse = eye + power
        power = by_block(power, power, every)
        for level in range(2):
            both = by_block(jnp.concatenate([power, inverse], axis=0), power, every)
            power = both[:HEAD]
            inverse = inverse + both[HEAD:]
        inverse = inverse + by_block(inverse, power, every)
        for link in links:
            inverse = inverse - by_block(
                by_block(inverse, jnp.where(link, mutual, 0.0), every), inverse, every
            )
        right = jnp.concatenate([probe[rows], by_block(value, through, every)], axis=0)
        basis = by_block(right, inverse, every)
        basis_ref[h] = basis
        taken = by_block(basis, removal_end[rows], every, turned=True)
        given = by_block(value, scaled_end[rows], every, turned=True)
        carry_maps = eye * block_decay[rows] - taken[:HEAD]
        carry_adds = given - taken[HEAD:]
        total = jnp.concatenate([carry_maps[:, :HEAD], carry_adds[:, :HEAD]], axis=0)
        prefix = [jnp.concatenate([eye[:, :HEAD], jnp.zeros((HEAD, HEAD), f32)], axis=0)]
        for b in range(1, BLOCKS):
            at = slice(b * BLOCK, (b + 1) * BLOCK)
            prefix.append(total)
            total = mm(total, carry_maps[:, at])
            total = jnp.concatenate([total[:HEAD], total[HEAD:] + carry_adds[:, at]], axis=0)
        prefix_ref[h] = jnp.concatenate(prefix, axis=1)
        pack_ref[rows, :] = jnp.concatenate([total[:HEAD], total[HEAD:]], axis=1).astype(bf16)


def reach_kernel(
    prefix_ref, basis_ref, removal_ref, scaled_ref, reads_ref, value_ref, state_ref, own_ref
):
    every = same_block().astype(bf16)
    row, col, block = compressed_iotas()
    upto = row <= col
    for h in range(GROUPS):
        rows = head_rows(h)
        reads = reads_ref[rows, :]
        removing, giving = reached(removal_ref[rows, :], scaled_ref[rows, :], reads, block)
        lost = by_block(basis_ref[h], jnp.where(upto, removing, 0.0), every)
        own = by_block(value_ref[rows, :], jnp.where(upto, giving, 0.0), every) - lost[HEAD:]
        both = by_block(prefix_ref[h], reads - lost[:HEAD], every)
        state_ref[rows, :] = both[:HEAD]
        own_ref[rows, :] = own + both[HEAD:]


def after_pack(total, pack):
    moved = mm(total, pack[:, :HEAD])
    return jnp.concatenate(
        [moved[:HEAD], moved[HEAD:] + pack[:, HEAD:].astype(f32)], axis=0
    )


def row_kernel(index_ref, own_ref, one_ref, two_ref, three_ref, pack_ref, before_ref, held):
    mine = index_ref[1]
    for shift, ref in enumerate((own_ref, one_ref, two_ref, three_ref)):
        held[(mine + 4 - shift) % 4] = ref[...]
    eye = (
        lax.broadcasted_iota(jnp.int32, (HEAD, HEAD), 0)
        == lax.broadcasted_iota(jnp.int32, (HEAD, HEAD), 1)
    ).astype(f32)
    start = jnp.concatenate([eye, jnp.zeros((HEAD, HEAD), f32)], axis=0)
    for h in range(GROUPS):
        rows = head_rows(h)
        members = [held[k, rows, :] for k in range(4)]
        first = jnp.concatenate(
            [members[0][:, :HEAD], members[0][:, HEAD:]], axis=0
        ).astype(f32)
        second = after_pack(first, members[1])
        third = after_pack(second, members[2])
        fourth = after_pack(third, members[3])
        before = jnp.where(
            mine == 0, start, jnp.where(mine == 1, first, jnp.where(mine == 2, second, third))
        )
        before_ref[h] = before
        pack_ref[rows, :] = jnp.concatenate([fourth[:HEAD], fourth[HEAD:]], axis=1).astype(bf16)


def window_kernel(two_ref, one_ref, own_ref, pack_ref):
    for h in range(GROUPS):
        rows = head_rows(h)
        first = two_ref[rows, :]
        total = jnp.concatenate([first[:, :HEAD], first[:, HEAD:]], axis=0)
        for ref in (one_ref, own_ref):
            total = after_pack(total, ref[rows, :])
        pack_ref[rows, :] = jnp.concatenate([total[:HEAD], total[HEAD:]], axis=1).astype(bf16)


def mixed_kernel(
    index_ref, six_ref, three_ref, two_ref, one_ref, before_ref, state_ref, own_ref, switch_ref, scaler_ref,
    keep_ref, send_ref, held,
):
    y = index_ref[2]
    core = index_ref[3]
    carried = [six_ref[head_rows(h), HEAD:].astype(f32) for h in range(GROUPS)]
    for ref in (three_ref, two_ref, one_ref):
        for h in range(GROUPS):
            member = ref[head_rows(h), :]
            carried[h] = mm(carried[h], member[:, :HEAD]) + member[:, HEAD:].astype(f32)
    heads = []
    for h in range(GROUPS):
        rows = head_rows(h)
        entering = mm(carried[h], before_ref[h, :HEAD]) + before_ref[h, HEAD:]
        outputs = mm(entering, state_ref[rows, :]) + own_ref[rows, :]
        centred = outputs - jnp.mean(outputs, axis=0, keepdims=True)
        heads.append(
            centred * lax.rsqrt(jnp.mean(centred * centred, axis=0, keepdims=True) + group_eps)
        )
    mixed = jnp.concatenate(heads, axis=0) * down_rows(scaler_ref[...], SPAN)
    mixed = mixed * switch_ref[...].astype(f32)
    held[...] = mixed.T.astype(bf16).reshape(8, 32, SPAN)
    for s in range(4):
        at = 2 * ((y + s) % 4)
        keep_ref[s] = held[at + core]
        send_ref[s] = held[at + 1 - core]


def project_kernel(keep_ref, got_ref, own_ref, other_ref, here_ref, one_ref, two_ref, three_ref):
    dot = functools.partial(jnp.dot, preferred_element_type=f32)
    rows = dot(keep_ref[...].reshape(128, SPAN), own_ref[...])
    rows = rows + dot(got_ref[...].reshape(128, SPAN), other_ref[...])
    here_ref[...] = rows[:32]
    one_ref[...] = rows[32:64].astype(bf16)
    two_ref[...] = rows[64:96].astype(bf16)
    three_ref[...] = rows[96:].astype(bf16)


VMEM = pl.BlockSpec(memory_space=pltpu.VMEM)
SMEM = pl.BlockSpec(memory_space=pltpu.SMEM)


def like(shape, kind=f32):
    return jax.ShapeDtypeStruct(shape, kind)


def whole(kernel, outs, *args, scratch=(), scalars=0, flops=0, name=None):
    specs = [SMEM] * scalars + [VMEM] * (len(args) - scalars)
    return pl.pallas_call(
        kernel,
        out_shape=outs,
        in_specs=specs,
        out_specs=jax.tree.map(lambda _: VMEM, outs),
        scratch_shapes=scratch,
        cost_estimate=pl.CostEstimate(flops=flops, transcendentals=0, bytes_accessed=1 << 20),
        name=name,
    )(*args)


def moved(x, axis, shift):
    size = lax.axis_size(axis)
    return lax.ppermute(x, axis, [(k, (k + shift) % size) for k in range(size)])


def carried_on(x, axis, shift):
    size = lax.axis_size(axis)
    return lax.ppermute(x, axis, [(k, k + shift) for k in range(size - shift)])


def rms_rows(middle, dense_block_scaler):
    scale_rows = lax.rsqrt(jnp.mean(middle * middle, axis=-1, keepdims=True) + norm_eps)
    return (middle * scale_rows * dense_block_scaler).astype(bf16)


def dense_kernel(*refs):
    rows_refs = refs[:8]
    weights_ref, keep_ref, send_ref, rows, weights, sems = refs[8:]
    count = sems.shape[0]
    chunk = weights.shape[0] // count
    copies = [
        pltpu.make_async_copy(
            weights_ref.at[pl.ds(k * chunk, chunk)], weights.at[pl.ds(k * chunk, chunk)], sems.at[k]
        )
        for k in range(count)
    ]
    for copy in copies:
        copy.start()
    for k, ref in enumerate(rows_refs):
        rows[32 * k : 32 * k + 32, :] = ref[...]
    width = weights.shape[1] // 3
    sums = None
    for k in range(count):
        copies[k].wait()
        at = slice(k * chunk, (k + 1) * chunk)
        part = jnp.dot(rows[:, at], weights[at, : 2 * width], preferred_element_type=f32)
        sums = part if sums is None else sums + part
    gate_sum = sums[:, :width]
    hidden = (gate_sum * sigmoid(gate_sum) * sums[:, width:]).astype(bf16)
    out = lax.dot_general(
        hidden, weights[:, 2 * width :], (((1,), (1,)), ((), ())), preferred_element_type=f32
    ).astype(bf16)
    keep_ref[...] = out[:128]
    send_ref[...] = out[128:]


def local(
    residual_matrix,
    query_vectors,
    lookup_vectors,
    payload_vectors,
    fading_dependent_term,
    step_size_preactivation,
    attention_result_switch,
    fading_bias_vector,
    surplus_forgetting,
    per_group_scaler,
    attention_result_matrix,
    dense_block_scaler,
    switching_matrix,
    expanding_matrix,
    contracting_matrix,
):
    index = jnp.stack([lax.axis_index(a) for a in ALL]).astype(jnp.int32)
    weights = lax.all_gather(
        jnp.concatenate([switching_matrix, expanding_matrix, contracting_matrix.T], axis=1),
        SP,
        axis=0,
        tiled=True,
    )
    other_matrix = moved(attention_result_matrix, "c", 1)
    full = like((SPAN, SPAN))
    wide = like((GROUPS, 2 * HEAD, SPAN))
    pack, *parts = whole(
        local_kernel,
        (like((SPAN, 128), bf16), wide, wide, full, full, full),
        lookup_vectors,
        payload_vectors,
        query_vectors,
        fading_dependent_term,
        step_size_preactivation,
        fading_bias_vector.reshape(1, -1),
        surplus_forgetting,
        flops=1 << 33,
        name="local",
    )
    others = [moved(pack, "x", s) for s in (1, 2, 3)]
    state, own = whole(
        reach_kernel, (full, full), *parts, payload_vectors, flops=1 << 32, name="reach",
    )
    row_pack, before = whole(
        row_kernel,
        (like((SPAN, 128), bf16), like((GROUPS, 128, HEAD))),
        index, pack, *others,
        scratch=[pltpu.VMEM((4, SPAN, 128), bf16)],
        scalars=1, flops=1 << 30, name="row",
    )
    near = [carried_on(row_pack, "z", s) for s in (2, 1)]
    window = whole(
        window_kernel, like((SPAN, 128), bf16), *near, row_pack, flops=1 << 30, name="window"
    )
    far = [carried_on(window, "z", s) for s in (6, 3)]
    keep, send = whole(
        mixed_kernel,
        (like((4, 32, SPAN), bf16), like((4, 32, SPAN), bf16)),
        index, *far, *near, before, state, own, attention_result_switch, per_group_scaler.reshape(1, -1),
        scratch=[pltpu.VMEM((8, 32, SPAN), bf16)],
        scalars=1, flops=1 << 30, name="mixed",
    )
    got = moved(send, "c", 1)
    here, *away = whole(
        project_kernel,
        (like((32, 2048)),) + (like((32, 2048), bf16),) * 3,
        keep, got, attention_result_matrix, other_matrix,
        flops=1 << 29, name="project",
    )
    middle = residual_matrix.astype(f32) + here
    for s, piece in enumerate(away, 1):
        middle = middle + moved(piece, "y", s).astype(f32)
    normed = rms_rows(middle, dense_block_scaler)
    mine = [normed] + [moved(normed, "y", s) for s in (1, 2, 3)]
    theirs = [moved(piece, "c", 1) for piece in mine]
    width = residual_matrix.shape[1]
    kept, sent = pl.pallas_call(
        dense_kernel,
        out_shape=(like((128, width), bf16), like((128, width), bf16)),
        in_specs=[VMEM] * 8 + [pl.BlockSpec(memory_space=pl.ANY)],
        out_specs=(VMEM, VMEM),
        scratch_shapes=[
            pltpu.VMEM((SPAN, width), bf16),
            pltpu.VMEM((width, weights.shape[1]), bf16),
            pltpu.SemaphoreType.DMA((4,)),
        ],
        name="dense",
    )(*mine, *theirs, weights)
    summed = kept.astype(f32) + moved(sent, "c", 1).astype(f32)
    channel_out = summed[:32]
    for s in (1, 2, 3):
        channel_out = channel_out + moved(
            summed[32 * s : 32 * s + 32].astype(bf16), "y", -s
        ).astype(f32)
    return (middle + channel_out).astype(bf16)


def solution(mesh):
    torus = Mesh(mesh.devices.reshape(8, 4, 4, 2), ALL)
    channels = P(TP, SP)
    placed = (
        P(ALL, None),
        channels,
        channels,
        channels,
        channels,
        channels,
        channels,
        P(TP),
        P(TP, SP),
        P(TP),
        P(TP, None),
        P(),
        P(SP, TP),
        P(SP, TP),
        P(TP, SP),
    )
    return jax.shard_map(
        local, mesh=torus, in_specs=placed, out_specs=P(ALL, None), check_vma=False
    )
```

```python
import functools

import jax
import jax.numpy as jnp
from jax import lax
from jax.experimental import pallas as pl
from jax.experimental.pallas import tpu as pltpu
from jax.sharding import Mesh
from jax.sharding import PartitionSpec as P

HEAD = 64
BLOCK = 64
GROUPS = 4
SPAN = 256
BLOCKS = SPAN // BLOCK
SP = ("z", "x")
TP = ("y", "c")
ALL = ("z", "x", "y", "c")

norm_eps = 1e-06
group_eps = 0.00064
key_eps = 1e-06
half_power = 0.6065306597126334

f32 = jnp.float32
bf16 = jnp.bfloat16


def pair(a):
    if a.dtype == bf16:
        return (a,)
    high = a.astype(bf16)
    return (high, (a - high.astype(f32)).astype(bf16))


def mm(a, b, dims=((1,), (0,))):
    a = a if isinstance(a, tuple) else pair(a)
    b = b if isinstance(b, tuple) else pair(b)
    dot = lambda l, r: lax.dot_general(l, r, (dims, ((), ())), preferred_element_type=f32)
    total = dot(a[0], b[0])
    if len(b) > 1:
        total = total + dot(a[0], b[1])
    if len(a) > 1:
        total = total + dot(a[1], b[0])
    return total


def sigmoid(x):
    return 1.0 / (1.0 + jnp.exp(-x))


def down_rows(row, width):
    turned = jnp.broadcast_to(row, (128, row.shape[1])).T
    return jnp.concatenate([turned] * (width // 128), axis=1)


def head_rows(h):
    return slice(h * HEAD, (h + 1) * HEAD)


def compressed_iotas():
    row = lax.broadcasted_iota(jnp.int32, (HEAD, SPAN), 0)
    lane = lax.broadcasted_iota(jnp.int32, (HEAD, SPAN), 1)
    return row, lane % BLOCK, lane // BLOCK


def same_block():
    row = lax.broadcasted_iota(jnp.int32, (SPAN, SPAN), 0) // BLOCK
    return jnp.where(row == lax.broadcasted_iota(jnp.int32, (SPAN, SPAN), 1) // BLOCK, 1.0, 0.0)


def spread(block, every):
    return jnp.concatenate([block] * BLOCKS, axis=0) * every


def by_block(left, right, every, turned=False):
    count = left.shape[0]
    dims = (((1,), (1,)) if turned else ((1,), (0,)), ((), ()))
    dot = lambda l, r: lax.dot_general(l, spread(r, every), dims, preferred_element_type=f32)
    left, right = pair(left), pair(right)
    if len(left) == 1:
        return dot(left[0], right[0]) + dot(left[0], right[1])
    both = dot(jnp.concatenate(left, axis=0), right[0])
    return both[:count] + both[count:] + dot(left[0], right[1])


def diagonal(full, block):
    total = jnp.where(block == 0, full[:HEAD], 0.0)
    for b in range(1, BLOCKS):
        total = total + jnp.where(block == b, full[b * HEAD : (b + 1) * HEAD], 0.0)
    return total


def reached(removal, scaled, seen, block):
    left = pair(jnp.concatenate([removal.T, scaled.T], axis=0))
    seen = pair(seen)
    dot = lambda l, r: jnp.dot(l, r, preferred_element_type=f32)
    both = dot(jnp.concatenate(left, axis=0), seen[0])
    both = both[: 2 * SPAN] + both[2 * SPAN :] + dot(left[0], seen[1])
    return diagonal(both[:SPAN], block), diagonal(both[SPAN:], block)


def local_kernel(
    key_ref, value_ref, query_ref, fading_ref, rate_ref, bias_ref, surplus_ref,
    pack_ref, prefix_ref, basis_ref, removal_ref, scaled_ref, reads_ref,
):
    every = same_block()
    row = lax.broadcasted_iota(jnp.int32, (SPAN, SPAN), 0)
    col = lax.broadcasted_iota(jnp.int32, (SPAN, SPAN), 1)
    upto = jnp.where(row <= col, every, 0.0).astype(bf16)
    every = every.astype(bf16)
    fading = fading_ref[...].astype(f32) + down_rows(bias_ref[...], SPAN)
    surplus = jnp.concatenate(
        [jnp.broadcast_to(surplus_ref[h : h + 1, :], (HEAD, SPAN)) for h in range(GROUPS)], axis=0
    )
    log_decay = surplus - half_power * sigmoid(fading)
    rate = sigmoid(rate_ref[...].astype(f32))
    keys = key_ref[...].astype(f32)
    norms = jnp.concatenate(
        [
            jnp.broadcast_to(
                lax.rsqrt(
                    jnp.sum(keys[head_rows(h)] * keys[head_rows(h)], axis=0, keepdims=True) + key_eps
                ),
                (HEAD, SPAN),
            )
            for h in range(GROUPS)
        ],
        axis=0,
    )
    unit = keys * norms
    scaled = keys * rate
    removal = unit * rate
    first = log_decay.astype(bf16)
    rest = log_decay - first.astype(f32)
    second = rest.astype(bf16)
    third = (rest - second.astype(f32)).astype(bf16)
    pieces = jnp.concatenate([first, second, third], axis=0)

    def running(m):
        sums = jnp.dot(pieces, m, preferred_element_type=f32)
        return sums[:SPAN] + sums[SPAN : 2 * SPAN] + sums[2 * SPAN :]

    after = running(upto)
    final = running(every)
    probe = unit * jnp.exp(after - log_decay)
    grow = jnp.exp(-after)
    removal_in = removal * grow
    scaled_in = scaled * grow
    end = jnp.exp(final - after)
    removal_end = removal * end
    scaled_end = scaled * end
    block_decay = jnp.exp(final)
    removal_ref[...] = removal_in
    scaled_ref[...] = scaled_in
    reads_ref[...] = query_ref[...].astype(f32) * jnp.exp(after)
    row, col, block = compressed_iotas()
    eye = (row == col).astype(f32)
    strict = row < col
    in16 = (row // 16) == (col // 16)
    in32 = (row // 32) == (col // 32)
    links = ((row // 16) != (col // 16)) & in32, ~in32
    heads = range(GROUPS)
    row_of = [head_rows(h) for h in heads]
    grams = [reached(removal_in[r], scaled_in[r], probe[r], block) for r in row_of]
    mutual = [jnp.where(strict, gram[0], 0.0) for gram in grams]
    through = [jnp.where(strict, gram[1], 0.0) for gram in grams]
    values = [value_ref[r, :] for r in row_of]
    power = [jnp.where(in16, -m, 0.0) for m in mutual]
    inverse = [eye + p for p in power]
    power = [by_block(p, p, every) for p in power]
    seen = [by_block(v, t, every) for v, t in zip(values, through)]
    given = [by_block(v, scaled_end[r], every, turned=True) for v, r in zip(values, row_of)]
    for level in range(2):
        both = [
            by_block(jnp.concatenate([p, i], axis=0), p, every) for p, i in zip(power, inverse)
        ]
        power = [two[:HEAD] for two in both]
        inverse = [i + two[HEAD:] for i, two in zip(inverse, both)]
    inverse = [i + by_block(i, p, every) for i, p in zip(inverse, power)]
    for link in links:
        bridge = [by_block(i, jnp.where(link, m, 0.0), every) for i, m in zip(inverse, mutual)]
        inverse = [i - by_block(k, i, every) for i, k in zip(inverse, bridge)]
    basis = [
        by_block(jnp.concatenate([probe[r], k], axis=0), i, every)
        for r, k, i in zip(row_of, seen, inverse)
    ]
    taken = [by_block(k, removal_end[r], every, turned=True) for k, r in zip(basis, row_of)]
    carry_maps = [eye * block_decay[r] - t[:HEAD] for r, t in zip(row_of, taken)]
    carry_adds = [g - t[HEAD:] for g, t in zip(given, taken)]
    total = [
        jnp.concatenate([m[:, :HEAD], k[:, :HEAD]], axis=0) for m, k in zip(carry_maps, carry_adds)
    ]
    start = jnp.concatenate([eye[:, :HEAD], jnp.zeros((HEAD, HEAD), f32)], axis=0)
    prefix = [[start] for h in heads]
    for b in range(1, BLOCKS):
        at = slice(b * BLOCK, (b + 1) * BLOCK)
        for h in heads:
            prefix[h].append(total[h])
        total = [mm(t, m[:, at]) for t, m in zip(total, carry_maps)]
        total = [
            jnp.concatenate([t[:HEAD], t[HEAD:] + k[:, at]], axis=0) for t, k in zip(total, carry_adds)
        ]
    for h in heads:
        pack_ref[row_of[h], :] = jnp.concatenate([total[h][:HEAD], total[h][HEAD:]], axis=1).astype(bf16)
        basis_ref[h] = basis[h]
        prefix_ref[h] = jnp.concatenate(prefix[h], axis=1)


def reach_kernel(
    prefix_ref, basis_ref, removal_ref, scaled_ref, reads_ref, value_ref, state_ref, own_ref
):
    every = same_block().astype(bf16)
    row, col, block = compressed_iotas()
    upto = row <= col
    row_of = [head_rows(h) for h in range(GROUPS)]
    reads = [reads_ref[r, :] for r in row_of]
    grams = [
        reached(removal_ref[r, :], scaled_ref[r, :], q, block) for r, q in zip(row_of, reads)
    ]
    lost = [
        by_block(basis_ref[h], jnp.where(upto, gram[0], 0.0), every) for h, gram in enumerate(grams)
    ]
    own = [
        by_block(value_ref[r, :], jnp.where(upto, gram[1], 0.0), every)
        for r, gram in zip(row_of, grams)
    ]
    both = [by_block(prefix_ref[h], reads[h] - lost[h][:HEAD], every) for h in range(GROUPS)]
    for h, r in enumerate(row_of):
        state_ref[r, :] = both[h][:HEAD]
        own_ref[r, :] = own[h] - lost[h][HEAD:] + both[h][HEAD:]


def after_pack(total, pack):
    moved = mm(total, pack[:, :HEAD])
    return jnp.concatenate(
        [moved[:HEAD], moved[HEAD:] + pack[:, HEAD:].astype(f32)], axis=0
    )


def row_kernel(index_ref, own_ref, one_ref, two_ref, three_ref, pack_ref, before_ref, held):
    mine = index_ref[1]
    for shift, ref in enumerate((own_ref, one_ref, two_ref, three_ref)):
        held[(mine + 4 - shift) % 4] = ref[...]
    eye = (
        lax.broadcasted_iota(jnp.int32, (HEAD, HEAD), 0)
        == lax.broadcasted_iota(jnp.int32, (HEAD, HEAD), 1)
    ).astype(f32)
    start = jnp.concatenate([eye, jnp.zeros((HEAD, HEAD), f32)], axis=0)
    heads = range(GROUPS)
    members = [[held[k, head_rows(h), :] for k in range(4)] for h in heads]
    first = [
        jnp.concatenate([m[0][:, :HEAD], m[0][:, HEAD:]], axis=0).astype(f32) for m in members
    ]
    second = [after_pack(f, m[1]) for f, m in zip(first, members)]
    third = [after_pack(f, m[2]) for f, m in zip(second, members)]
    fourth = [after_pack(f, m[3]) for f, m in zip(third, members)]
    for h in heads:
        before_ref[h] = jnp.where(
            mine == 0, start, jnp.where(mine == 1, first[h], jnp.where(mine == 2, second[h], third[h]))
        )
        pack_ref[head_rows(h), :] = jnp.concatenate(
            [fourth[h][:HEAD], fourth[h][HEAD:]], axis=1
        ).astype(bf16)


def window_kernel(two_ref, one_ref, own_ref, pack_ref):
    row_of = [head_rows(h) for h in range(GROUPS)]
    total = [
        jnp.concatenate([two_ref[r, :HEAD], two_ref[r, HEAD:]], axis=0) for r in row_of
    ]
    for ref in (one_ref, own_ref):
        total = [after_pack(t, ref[r, :]) for t, r in zip(total, row_of)]
    for t, r in zip(total, row_of):
        pack_ref[r, :] = jnp.concatenate([t[:HEAD], t[HEAD:]], axis=1).astype(bf16)


def mixed_kernel(
    index_ref, six_ref, three_ref, two_ref, one_ref, before_ref, state_ref, own_ref, switch_ref, scaler_ref,
    keep_ref, send_ref, held,
):
    y = index_ref[2]
    core = index_ref[3]
    carried = [six_ref[head_rows(h), HEAD:].astype(f32) for h in range(GROUPS)]
    for ref in (three_ref, two_ref, one_ref):
        for h in range(GROUPS):
            member = ref[head_rows(h), :]
            carried[h] = mm(carried[h], member[:, :HEAD]) + member[:, HEAD:].astype(f32)
    row_of = [head_rows(h) for h in range(GROUPS)]
    entering = [
        mm(carried[h], before_ref[h, :HEAD]) + before_ref[h, HEAD:] for h in range(GROUPS)
    ]
    outputs = [mm(e, state_ref[r, :]) + own_ref[r, :] for e, r in zip(entering, row_of)]
    centred = [o - jnp.mean(o, axis=0, keepdims=True) for o in outputs]
    heads = [
        k * lax.rsqrt(jnp.mean(k * k, axis=0, keepdims=True) + group_eps) for k in centred
    ]
    mixed = jnp.concatenate(heads, axis=0) * down_rows(scaler_ref[...], SPAN)
    mixed = mixed * switch_ref[...].astype(f32)
    held[...] = mixed.T.astype(bf16).reshape(8, 32, SPAN)
    for s in range(4):
        at = 2 * ((y + s) % 4)
        keep_ref[s] = held[at + core]
        send_ref[s] = held[at + 1 - core]


def project_kernel(keep_ref, got_ref, own_ref, other_ref, here_ref, one_ref, two_ref, three_ref):
    dot = functools.partial(jnp.dot, preferred_element_type=f32)
    rows = dot(keep_ref[...].reshape(128, SPAN), own_ref[...])
    rows = rows + dot(got_ref[...].reshape(128, SPAN), other_ref[...])
    here_ref[...] = rows[:32]
    one_ref[...] = rows[32:64].astype(bf16)
    two_ref[...] = rows[64:96].astype(bf16)
    three_ref[...] = rows[96:].astype(bf16)


VMEM = pl.BlockSpec(memory_space=pltpu.VMEM)
SMEM = pl.BlockSpec(memory_space=pltpu.SMEM)


def like(shape, kind=f32):
    return jax.ShapeDtypeStruct(shape, kind)


def whole(kernel, outs, *args, scratch=(), scalars=0, flops=0, name=None):
    specs = [SMEM] * scalars + [VMEM] * (len(args) - scalars)
    return pl.pallas_call(
        kernel,
        out_shape=outs,
        in_specs=specs,
        out_specs=jax.tree.map(lambda _: VMEM, outs),
        scratch_shapes=scratch,
        cost_estimate=pl.CostEstimate(flops=flops, transcendentals=0, bytes_accessed=1 << 20),
        name=name,
    )(*args)


def moved(x, axis, shift):
    size = lax.axis_size(axis)
    return lax.ppermute(x, axis, [(k, (k + shift) % size) for k in range(size)])


def carried_on(x, axis, shift):
    size = lax.axis_size(axis)
    return lax.ppermute(x, axis, [(k, k + shift) for k in range(size - shift)])


def rms_rows(middle, dense_block_scaler):
    scale_rows = lax.rsqrt(jnp.mean(middle * middle, axis=-1, keepdims=True) + norm_eps)
    return (middle * scale_rows * dense_block_scaler).astype(bf16)


def dense_kernel(width, index_ref, *refs):
    rows_refs = refs[:4]
    near_ref, far_ref, out_refs = refs[4], refs[5], refs[6:10]
    rows, weights, sems = refs[10:]
    half = index_ref[1] // 2
    core = index_ref[3]
    copies = []
    for z in range(8):
        copies.append([])
        for ref, parity in ((near_ref, core), (far_ref, 1 - core)):
            for k in range(2):
                to = HEAD * (4 * z + 2 * ((half + k) % 2) + parity)
                copies[-1].append(
                    pltpu.make_async_copy(
                        ref.at[pl.ds(2 * HEAD * z + HEAD * k, HEAD)],
                        weights.at[pl.ds(pl.multiple_of(to, HEAD), HEAD)],
                        sems.at[z],
                    )
                )
    for group in copies:
        for copy in group:
            copy.start()
    each = rows_refs[0].shape[0]
    for k, ref in enumerate(rows_refs):
        rows[each * k : each * k + each, :] = ref[...]
    sums = None
    for z in range(8):
        for copy in copies[z]:
            copy.wait()
        if z % 2 == 0:
            continue
        at = slice((z - 1) * SPAN, (z + 1) * SPAN)
        part = jnp.dot(rows[:, at], weights[at, : 2 * width], preferred_element_type=f32)
        sums = part if sums is None else sums + part
    gate_sum = sums[:, :width]
    hidden = (gate_sum * sigmoid(gate_sum) * sums[:, width:]).astype(bf16)
    out = lax.dot_general(
        hidden, weights[:, 2 * width : 3 * width], (((1,), (1,)), ((), ())), preferred_element_type=f32
    ).astype(bf16)
    for k, ref in enumerate(out_refs):
        ref[...] = out[each * k : each * k + each]


def across(x):
    return lax.ppermute(x, "x", [(k, k ^ 1) for k in range(4)])


def to_parity(x, flip):
    pairs = []
    for place in range(4):
        for core in range(2):
            chip = core + 2 * ((place // 2) ^ flip)
            pairs.append((2 * place + core, 2 * chip + place % 2))
    return lax.ppermute(x, ("x", "c"), pairs)


def local(
    residual_matrix,
    query_vectors,
    lookup_vectors,
    payload_vectors,
    fading_dependent_term,
    step_size_preactivation,
    attention_result_switch,
    fading_bias_vector,
    surplus_forgetting,
    per_group_scaler,
    attention_result_matrix,
    dense_block_scaler,
    switching_matrix,
    expanding_matrix,
    contracting_matrix,
):
    index = jnp.stack([lax.axis_index(a) for a in ALL]).astype(jnp.int32)
    hidden_width = switching_matrix.shape[1]
    blank = jnp.zeros((switching_matrix.shape[0], -3 * hidden_width % 128), bf16)
    shard = jnp.concatenate(
        [switching_matrix, expanding_matrix, contracting_matrix.T, blank], axis=1
    )
    arriving = (to_parity(shard, 0), to_parity(shard, 1))
    other_matrix = moved(attention_result_matrix, "c", 1)
    full = like((SPAN, SPAN))
    wide = like((GROUPS, 2 * HEAD, SPAN))
    pack, *parts = whole(
        local_kernel,
        (like((SPAN, 128), bf16), wide, wide, full, full, full),
        lookup_vectors,
        payload_vectors,
        query_vectors,
        fading_dependent_term,
        step_size_preactivation,
        fading_bias_vector.reshape(1, -1),
        surplus_forgetting,
        flops=1 << 33,
        name="local",
    )
    *arrived, _ = lax.optimization_barrier((*arriving, pack))
    near = lax.all_gather(jnp.concatenate(arrived, axis=0), "z", axis=0, tiled=True)
    others = [moved(pack, "x", s) for s in (1, 2, 3)]
    state, own = whole(
        reach_kernel, (full, full), *parts, payload_vectors, flops=1 << 32, name="reach",
    )
    row_pack, before = whole(
        row_kernel,
        (like((SPAN, 128), bf16), like((GROUPS, 128, HEAD))),
        index, pack, *others,
        scratch=[pltpu.VMEM((4, SPAN, 128), bf16)],
        scalars=1, flops=1 << 30, name="row",
    )
    close = [carried_on(row_pack, "z", s) for s in (2, 1)]
    window = whole(
        window_kernel, like((SPAN, 128), bf16), *close, row_pack, flops=1 << 30, name="window"
    )
    distant = [carried_on(window, "z", s) for s in (6, 3)]
    keep, send = whole(
        mixed_kernel,
        (like((4, 32, SPAN), bf16), like((4, 32, SPAN), bf16)),
        index, *distant, *close, before, state, own, attention_result_switch, per_group_scaler.reshape(1, -1),
        scratch=[pltpu.VMEM((8, 32, SPAN), bf16)],
        scalars=1, flops=1 << 30, name="mixed",
    )
    got = moved(send, "c", 1)
    here, *away = whole(
        project_kernel,
        (like((32, 2048)),) + (like((32, 2048), bf16),) * 3,
        keep, got, attention_result_matrix, other_matrix,
        flops=1 << 29, name="project",
    )
    middle = residual_matrix.astype(f32) + here
    for s, piece in enumerate(away, 1):
        middle = middle + moved(piece, "y", s).astype(f32)
    normed = rms_rows(middle, dense_block_scaler)
    both = jnp.concatenate([normed, across(normed)], axis=0)
    own_half, _ = lax.optimization_barrier((near, both))
    far = moved(own_half, "c", 1)
    rows = [both] + [moved(both, "y", s) for s in (1, 2, 3)]
    width = normed.shape[1]
    parts = pl.pallas_call(
        functools.partial(dense_kernel, hidden_width),
        out_shape=(like(both.shape, bf16),) * 4,
        in_specs=[SMEM] + [VMEM] * 4 + [pl.BlockSpec(memory_space=pl.ANY)] * 2,
        out_specs=(VMEM,) * 4,
        scratch_shapes=[
            pltpu.VMEM((SPAN, width), bf16),
            pltpu.VMEM((width, near.shape[1]), bf16),
            pltpu.SemaphoreType.DMA((8,)),
        ],
        name="dense",
    )(index, *rows, near, far)
    pair_out = parts[0].astype(f32)
    for s in (1, 2, 3):
        pair_out = pair_out + moved(parts[s], "y", -s).astype(f32)
    channel_out = pair_out[:32] + across(pair_out[32:].astype(bf16)).astype(f32)
    return (middle + channel_out).astype(bf16)


def solution(mesh):
    torus = Mesh(mesh.devices.reshape(8, 4, 4, 2), ALL)
    channels = P(TP, SP)
    placed = (
        P(ALL, None),
        channels,
        channels,
        channels,
        channels,
        channels,
        channels,
        P(TP),
        P(TP, SP),
        P(TP),
        P(TP, None),
        P(),
        P(SP, TP),
        P(SP, TP),
        P(TP, SP),
    )
    return jax.shard_map(
        local, mesh=torus, in_specs=placed, out_specs=P(ALL, None), check_vma=False
    )
```

```python
import functools

import jax
import jax.numpy as jnp
from jax import lax
from jax.experimental import pallas as pl
from jax.experimental.pallas import tpu as pltpu
from jax.sharding import Mesh
from jax.sharding import PartitionSpec as P

HEAD = 64
BLOCK = 64
GROUPS = 4
SPAN = 256
BLOCKS = SPAN // BLOCK
SP = ("z", "x")
TP = ("y", "c")
ALL = ("z", "x", "y", "c")

norm_eps = 1e-06
group_eps = 0.00064
key_eps = 1e-06
half_power = 0.6065306597126334

f32 = jnp.float32
bf16 = jnp.bfloat16


def pair(a):
    if a.dtype == bf16:
        return (a,)
    high = a.astype(bf16)
    return (high, (a - high.astype(f32)).astype(bf16))


def mm(a, b, dims=((1,), (0,))):
    a = a if isinstance(a, tuple) else pair(a)
    b = b if isinstance(b, tuple) else pair(b)
    dot = lambda l, r: lax.dot_general(l, r, (dims, ((), ())), preferred_element_type=f32)
    total = dot(a[0], b[0])
    if len(b) > 1:
        total = total + dot(a[0], b[1])
    if len(a) > 1:
        total = total + dot(a[1], b[0])
    return total


def sigmoid(x):
    return 1.0 / (1.0 + jnp.exp(-x))


def down_rows(row, width):
    turned = jnp.broadcast_to(row, (128, row.shape[1])).T
    return jnp.concatenate([turned] * (width // 128), axis=1)


def head_rows(h):
    return slice(h * HEAD, (h + 1) * HEAD)


def compressed_iotas():
    row = lax.broadcasted_iota(jnp.int32, (HEAD, SPAN), 0)
    lane = lax.broadcasted_iota(jnp.int32, (HEAD, SPAN), 1)
    return row, lane % BLOCK, lane // BLOCK


def same_block():
    row = lax.broadcasted_iota(jnp.int32, (SPAN, SPAN), 0) // BLOCK
    return jnp.where(row == lax.broadcasted_iota(jnp.int32, (SPAN, SPAN), 1) // BLOCK, 1.0, 0.0)


def spread(block, every):
    return jnp.concatenate([block] * BLOCKS, axis=0) * every


def by_block(left, right, every, turned=False):
    count = left.shape[0]
    dims = (((1,), (1,)) if turned else ((1,), (0,)), ((), ()))
    dot = lambda l, r: lax.dot_general(l, spread(r, every), dims, preferred_element_type=f32)
    left, right = pair(left), pair(right)
    if len(left) == 1:
        return dot(left[0], right[0]) + dot(left[0], right[1])
    both = dot(jnp.concatenate(left, axis=0), right[0])
    return both[:count] + both[count:] + dot(left[0], right[1])


def diagonal(full, block):
    total = jnp.where(block == 0, full[:HEAD], 0.0)
    for b in range(1, BLOCKS):
        total = total + jnp.where(block == b, full[b * HEAD : (b + 1) * HEAD], 0.0)
    return total


def reached(removal, scaled, seen, block):
    left = pair(jnp.concatenate([removal.T, scaled.T], axis=0))
    seen = pair(seen)
    dot = lambda l, r: jnp.dot(l, r, preferred_element_type=f32)
    both = dot(jnp.concatenate(left, axis=0), seen[0])
    both = both[: 2 * SPAN] + both[2 * SPAN :] + dot(left[0], seen[1])
    return diagonal(both[:SPAN], block), diagonal(both[SPAN:], block)


def local_kernel(
    key_ref, value_ref, query_ref, fading_ref, rate_ref, bias_ref, surplus_ref,
    pack_ref, prefix_ref, basis_ref, removal_ref, scaled_ref, reads_ref,
):
    every = same_block()
    row = lax.broadcasted_iota(jnp.int32, (SPAN, SPAN), 0)
    col = lax.broadcasted_iota(jnp.int32, (SPAN, SPAN), 1)
    upto = jnp.where(row <= col, every, 0.0).astype(bf16)
    every = every.astype(bf16)
    fading = fading_ref[...].astype(f32) + down_rows(bias_ref[...], SPAN)
    surplus = jnp.concatenate(
        [jnp.broadcast_to(surplus_ref[h : h + 1, :], (HEAD, SPAN)) for h in range(GROUPS)], axis=0
    )
    log_decay = surplus - half_power * sigmoid(fading)
    rate = sigmoid(rate_ref[...].astype(f32))
    keys = key_ref[...].astype(f32)
    norms = jnp.concatenate(
        [
            jnp.broadcast_to(
                lax.rsqrt(
                    jnp.sum(keys[head_rows(h)] * keys[head_rows(h)], axis=0, keepdims=True) + key_eps
                ),
                (HEAD, SPAN),
            )
            for h in range(GROUPS)
        ],
        axis=0,
    )
    unit = keys * norms
    scaled = keys * rate
    removal = unit * rate
    first = log_decay.astype(bf16)
    rest = log_decay - first.astype(f32)
    second = rest.astype(bf16)
    third = (rest - second.astype(f32)).astype(bf16)
    pieces = jnp.concatenate([first, second, third], axis=0)

    def running(m):
        sums = jnp.dot(pieces, m, preferred_element_type=f32)
        return sums[:SPAN] + sums[SPAN : 2 * SPAN] + sums[2 * SPAN :]

    after = running(upto)
    final = running(every)
    probe = unit * jnp.exp(after - log_decay)
    grow = jnp.exp(-after)
    removal_in = removal * grow
    scaled_in = scaled * grow
    end = jnp.exp(final - after)
    removal_end = removal * end
    scaled_end = scaled * end
    block_decay = jnp.exp(final)
    removal_ref[...] = removal_in
    scaled_ref[...] = scaled_in
    reads_ref[...] = query_ref[...].astype(f32) * jnp.exp(after)
    row, col, block = compressed_iotas()
    eye = (row == col).astype(f32)
    strict = row < col
    in16 = (row // 16) == (col // 16)
    in32 = (row // 32) == (col // 32)
    links = ((row // 16) != (col // 16)) & in32, ~in32
    heads = range(GROUPS)
    row_of = [head_rows(h) for h in heads]
    grams = [reached(removal_in[r], scaled_in[r], probe[r], block) for r in row_of]
    mutual = [jnp.where(strict, gram[0], 0.0) for gram in grams]
    through = [jnp.where(strict, gram[1], 0.0) for gram in grams]
    values = [value_ref[r, :] for r in row_of]
    power = [jnp.where(in16, -m, 0.0) for m in mutual]
    inverse = [eye + p for p in power]
    power = [by_block(p, p, every) for p in power]
    seen = [by_block(v, t, every) for v, t in zip(values, through)]
    given = [by_block(v, scaled_end[r], every, turned=True) for v, r in zip(values, row_of)]
    for level in range(2):
        both = [
            by_block(jnp.concatenate([p, i], axis=0), p, every) for p, i in zip(power, inverse)
        ]
        power = [two[:HEAD] for two in both]
        inverse = [i + two[HEAD:] for i, two in zip(inverse, both)]
    inverse = [i + by_block(i, p, every) for i, p in zip(inverse, power)]
    for link in links:
        bridge = [by_block(i, jnp.where(link, m, 0.0), every) for i, m in zip(inverse, mutual)]
        inverse = [i - by_block(k, i, every) for i, k in zip(inverse, bridge)]
    basis = [
        by_block(jnp.concatenate([probe[r], k], axis=0), i, every)
        for r, k, i in zip(row_of, seen, inverse)
    ]
    taken = [by_block(k, removal_end[r], every, turned=True) for k, r in zip(basis, row_of)]
    carry_maps = [eye * block_decay[r] - t[:HEAD] for r, t in zip(row_of, taken)]
    carry_adds = [g - t[HEAD:] for g, t in zip(given, taken)]
    total = [
        jnp.concatenate([m[:, :HEAD], k[:, :HEAD]], axis=0) for m, k in zip(carry_maps, carry_adds)
    ]
    start = jnp.concatenate([eye[:, :HEAD], jnp.zeros((HEAD, HEAD), f32)], axis=0)
    prefix = [[start] for h in heads]
    for b in range(1, BLOCKS):
        at = slice(b * BLOCK, (b + 1) * BLOCK)
        for h in heads:
            prefix[h].append(total[h])
        total = [mm(t, m[:, at]) for t, m in zip(total, carry_maps)]
        total = [
            jnp.concatenate([t[:HEAD], t[HEAD:] + k[:, at]], axis=0) for t, k in zip(total, carry_adds)
        ]
    for h in heads:
        pack_ref[row_of[h], :] = jnp.concatenate([total[h][:HEAD], total[h][HEAD:]], axis=1).astype(bf16)
        basis_ref[h] = basis[h]
        prefix_ref[h] = jnp.concatenate(prefix[h], axis=1)


def reach_kernel(
    prefix_ref, basis_ref, removal_ref, scaled_ref, reads_ref, value_ref, state_ref, own_ref
):
    every = same_block().astype(bf16)
    row, col, block = compressed_iotas()
    upto = row <= col
    row_of = [head_rows(h) for h in range(GROUPS)]
    reads = [reads_ref[r, :] for r in row_of]
    grams = [
        reached(removal_ref[r, :], scaled_ref[r, :], q, block) for r, q in zip(row_of, reads)
    ]
    lost = [
        by_block(basis_ref[h], jnp.where(upto, gram[0], 0.0), every) for h, gram in enumerate(grams)
    ]
    own = [
        by_block(value_ref[r, :], jnp.where(upto, gram[1], 0.0), every)
        for r, gram in zip(row_of, grams)
    ]
    both = [by_block(prefix_ref[h], reads[h] - lost[h][:HEAD], every) for h in range(GROUPS)]
    for h, r in enumerate(row_of):
        state_ref[r, :] = both[h][:HEAD]
        own_ref[r, :] = own[h] - lost[h][HEAD:] + both[h][HEAD:]


def after_pack(total, pack):
    moved = mm(total, pack[:, :HEAD])
    return jnp.concatenate(
        [moved[:HEAD], moved[HEAD:] + pack[:, HEAD:].astype(f32)], axis=0
    )


def row_kernel(index_ref, own_ref, one_ref, two_ref, three_ref, pack_ref, before_ref, held):
    mine = index_ref[1]
    for shift, ref in enumerate((own_ref, one_ref, two_ref, three_ref)):
        held[(mine + 4 - shift) % 4] = ref[...]
    eye = (
        lax.broadcasted_iota(jnp.int32, (HEAD, HEAD), 0)
        == lax.broadcasted_iota(jnp.int32, (HEAD, HEAD), 1)
    ).astype(f32)
    start = jnp.concatenate([eye, jnp.zeros((HEAD, HEAD), f32)], axis=0)
    heads = range(GROUPS)
    members = [[held[k, head_rows(h), :] for k in range(4)] for h in heads]
    first = [
        jnp.concatenate([m[0][:, :HEAD], m[0][:, HEAD:]], axis=0).astype(f32) for m in members
    ]
    second = [after_pack(f, m[1]) for f, m in zip(first, members)]
    third = [after_pack(f, m[2]) for f, m in zip(second, members)]
    fourth = [after_pack(f, m[3]) for f, m in zip(third, members)]
    for h in heads:
        before_ref[h] = jnp.where(
            mine == 0, start, jnp.where(mine == 1, first[h], jnp.where(mine == 2, second[h], third[h]))
        )
        pack_ref[head_rows(h), :] = jnp.concatenate(
            [fourth[h][:HEAD], fourth[h][HEAD:]], axis=1
        ).astype(bf16)


def window_kernel(two_ref, one_ref, own_ref, pack_ref):
    row_of = [head_rows(h) for h in range(GROUPS)]
    total = [
        jnp.concatenate([two_ref[r, :HEAD], two_ref[r, HEAD:]], axis=0) for r in row_of
    ]
    for ref in (one_ref, own_ref):
        total = [after_pack(t, ref[r, :]) for t, r in zip(total, row_of)]
    for t, r in zip(total, row_of):
        pack_ref[r, :] = jnp.concatenate([t[:HEAD], t[HEAD:]], axis=1).astype(bf16)


def mixed_kernel(
    index_ref, six_ref, three_ref, two_ref, one_ref, before_ref, state_ref, own_ref, switch_ref, scaler_ref,
    keep_ref, send_ref, held,
):
    y = index_ref[2]
    core = index_ref[3]
    carried = [six_ref[head_rows(h), HEAD:].astype(f32) for h in range(GROUPS)]
    for ref in (three_ref, two_ref, one_ref):
        for h in range(GROUPS):
            member = ref[head_rows(h), :]
            carried[h] = mm(carried[h], member[:, :HEAD]) + member[:, HEAD:].astype(f32)
    row_of = [head_rows(h) for h in range(GROUPS)]
    entering = [
        mm(carried[h], before_ref[h, :HEAD]) + before_ref[h, HEAD:] for h in range(GROUPS)
    ]
    outputs = [mm(e, state_ref[r, :]) + own_ref[r, :] for e, r in zip(entering, row_of)]
    centred = [o - jnp.mean(o, axis=0, keepdims=True) for o in outputs]
    heads = [
        k * lax.rsqrt(jnp.mean(k * k, axis=0, keepdims=True) + group_eps) for k in centred
    ]
    mixed = jnp.concatenate(heads, axis=0) * down_rows(scaler_ref[...], SPAN)
    mixed = mixed * switch_ref[...].astype(f32)
    held[...] = mixed.T.astype(bf16).reshape(8, 32, SPAN)
    for s in range(4):
        at = 2 * ((y + s) % 4)
        keep_ref[s] = held[at + core]
        send_ref[s] = held[at + 1 - core]


def project_kernel(keep_ref, got_ref, own_ref, other_ref, here_ref, one_ref, two_ref, three_ref):
    dot = functools.partial(jnp.dot, preferred_element_type=f32)
    rows = dot(keep_ref[...].reshape(128, SPAN), own_ref[...])
    rows = rows + dot(got_ref[...].reshape(128, SPAN), other_ref[...])
    here_ref[...] = rows[:32]
    one_ref[...] = rows[32:64].astype(bf16)
    two_ref[...] = rows[64:96].astype(bf16)
    three_ref[...] = rows[96:].astype(bf16)


VMEM = pl.BlockSpec(memory_space=pltpu.VMEM)
SMEM = pl.BlockSpec(memory_space=pltpu.SMEM)


def like(shape, kind=f32):
    return jax.ShapeDtypeStruct(shape, kind)


def whole(kernel, outs, *args, scratch=(), scalars=0, flops=0, name=None):
    specs = [SMEM] * scalars + [VMEM] * (len(args) - scalars)
    return pl.pallas_call(
        kernel,
        out_shape=outs,
        in_specs=specs,
        out_specs=jax.tree.map(lambda _: VMEM, outs),
        scratch_shapes=scratch,
        cost_estimate=pl.CostEstimate(flops=flops, transcendentals=0, bytes_accessed=1 << 20),
        name=name,
    )(*args)


def moved(x, axis, shift):
    size = lax.axis_size(axis)
    return lax.ppermute(x, axis, [(k, (k + shift) % size) for k in range(size)])


def carried_on(x, axis, shift):
    size = lax.axis_size(axis)
    return lax.ppermute(x, axis, [(k, k + shift) for k in range(size - shift)])


def rms_rows(middle, dense_block_scaler):
    scale_rows = lax.rsqrt(jnp.mean(middle * middle, axis=-1, keepdims=True) + norm_eps)
    return (middle * scale_rows * dense_block_scaler).astype(bf16)


def dense_kernel(width, index_ref, *refs):
    rows_refs = refs[:5]
    near_ref, far_ref, out_refs = refs[5], refs[6], refs[7:12]
    rows, weights, sems = refs[12:]
    half = index_ref[1] // 2
    core = index_ref[3]
    copies = []
    for z in range(8):
        copies.append([])
        for ref, parity in ((near_ref, core), (far_ref, 1 - core)):
            for k in range(2):
                to = HEAD * (4 * z + 2 * ((half + k) % 2) + parity)
                copies[-1].append(
                    pltpu.make_async_copy(
                        ref.at[pl.ds(2 * HEAD * z + HEAD * k, HEAD)],
                        weights.at[pl.ds(pl.multiple_of(to, HEAD), HEAD)],
                        sems.at[z],
                    )
                )
    for group in copies:
        for copy in group:
            copy.start()
    places = []
    for ref in rows_refs:
        at = places[-1].stop if places else 0
        places.append(slice(at, at + ref.shape[0]))
        rows[places[-1], :] = ref[...]
    sums = None
    for z in range(8):
        for copy in copies[z]:
            copy.wait()
        if z % 2 == 0:
            continue
        at = slice((z - 1) * SPAN, (z + 1) * SPAN)
        part = jnp.dot(rows[:, at], weights[at, : 2 * width], preferred_element_type=f32)
        sums = part if sums is None else sums + part
    gate_sum = sums[:, :width]
    hidden = (gate_sum * sigmoid(gate_sum) * sums[:, width:]).astype(bf16)
    out = lax.dot_general(
        hidden, weights[:, 2 * width : 3 * width], (((1,), (1,)), ((), ())), preferred_element_type=f32
    ).astype(bf16)
    for place, ref in zip(places, out_refs):
        ref[...] = out[place]


def across(x):
    return lax.ppermute(x, "x", [(k, k ^ 1) for k in range(4)])


def to_parity(x, flip):
    pairs = []
    for place in range(4):
        for core in range(2):
            chip = core + 2 * ((place // 2) ^ flip)
            pairs.append((2 * place + core, 2 * chip + place % 2))
    return lax.ppermute(x, ("x", "c"), pairs)


def local(
    residual_matrix,
    query_vectors,
    lookup_vectors,
    payload_vectors,
    fading_dependent_term,
    step_size_preactivation,
    attention_result_switch,
    fading_bias_vector,
    surplus_forgetting,
    per_group_scaler,
    attention_result_matrix,
    dense_block_scaler,
    switching_matrix,
    expanding_matrix,
    contracting_matrix,
):
    index = jnp.stack([lax.axis_index(a) for a in ALL]).astype(jnp.int32)
    hidden_width = switching_matrix.shape[1]
    blank = jnp.zeros((switching_matrix.shape[0], -3 * hidden_width % 128), bf16)
    shard = jnp.concatenate(
        [switching_matrix, expanding_matrix, contracting_matrix.T, blank], axis=1
    )
    arriving = (to_parity(shard, 0), to_parity(shard, 1))
    other_matrix = moved(attention_result_matrix, "c", 1)
    full = like((SPAN, SPAN))
    wide = like((GROUPS, 2 * HEAD, SPAN))
    pack, *parts = whole(
        local_kernel,
        (like((SPAN, 128), bf16), wide, wide, full, full, full),
        lookup_vectors,
        payload_vectors,
        query_vectors,
        fading_dependent_term,
        step_size_preactivation,
        fading_bias_vector.reshape(1, -1),
        surplus_forgetting,
        flops=1 << 33,
        name="local",
    )
    *arrived, _ = lax.optimization_barrier((*arriving, pack))
    near = lax.all_gather(jnp.concatenate(arrived, axis=0), "z", axis=0, tiled=True)
    others = [moved(pack, "x", s) for s in (1, 2, 3)]
    state, own = whole(
        reach_kernel, (full, full), *parts, payload_vectors, flops=1 << 32, name="reach",
    )
    row_pack, before = whole(
        row_kernel,
        (like((SPAN, 128), bf16), like((GROUPS, 128, HEAD))),
        index, pack, *others,
        scratch=[pltpu.VMEM((4, SPAN, 128), bf16)],
        scalars=1, flops=1 << 30, name="row",
    )
    close = [carried_on(row_pack, "z", s) for s in (2, 1)]
    window = whole(
        window_kernel, like((SPAN, 128), bf16), *close, row_pack, flops=1 << 30, name="window"
    )
    distant = [carried_on(window, "z", s) for s in (6, 3)]
    keep, send = whole(
        mixed_kernel,
        (like((4, 32, SPAN), bf16), like((4, 32, SPAN), bf16)),
        index, *distant, *close, before, state, own, attention_result_switch, per_group_scaler.reshape(1, -1),
        scratch=[pltpu.VMEM((8, 32, SPAN), bf16)],
        scalars=1, flops=1 << 30, name="mixed",
    )
    got = moved(send, "c", 1)
    here, *away = whole(
        project_kernel,
        (like((32, 2048)),) + (like((32, 2048), bf16),) * 3,
        keep, got, attention_result_matrix, other_matrix,
        flops=1 << 29, name="project",
    )
    middle = residual_matrix.astype(f32) + here
    for s, piece in enumerate(away, 1):
        middle = middle + moved(piece, "y", s).astype(f32)
    normed = rms_rows(middle, dense_block_scaler)
    both = jnp.concatenate([normed, across(normed)], axis=0)
    own_half, _ = lax.optimization_barrier((near, both))
    far = moved(own_half, "c", 1)
    half = normed.shape[0]
    ahead = moved(both, "y", 1)
    behind = moved(both, "y", -1)
    rows = [both, ahead, behind, moved(ahead[:half], "y", 1), moved(behind[half:], "y", -1)]
    width = normed.shape[1]
    parts = pl.pallas_call(
        functools.partial(dense_kernel, hidden_width),
        out_shape=tuple(like(part.shape, bf16) for part in rows),
        in_specs=[SMEM] + [VMEM] * 7,
        out_specs=(VMEM,) * 5,
        scratch_shapes=[
            pltpu.VMEM((SPAN, width), bf16),
            pltpu.VMEM((width, near.shape[1]), bf16),
            pltpu.SemaphoreType.DMA((8,)),
        ],
        compiler_params=pltpu.CompilerParams(vmem_limit_bytes=40 << 20),
        name="dense",
    )(index, *rows, near, far)
    own, low, high, low_half, high_half = [part.astype(f32) for part in parts]
    below = moved(parts[3], "y", -1).astype(f32)
    above = moved(parts[4], "y", 1).astype(f32)
    low = jnp.concatenate([low[:half] + below, low[half:]], axis=0).astype(bf16)
    high = jnp.concatenate([high[:half], high[half:] + above], axis=0).astype(bf16)
    pair_out = own + moved(low, "y", -1).astype(f32) + moved(high, "y", 1).astype(f32)
    channel_out = pair_out[:32] + across(pair_out[32:].astype(bf16)).astype(f32)
    return (middle + channel_out).astype(bf16)


def solution(mesh):
    torus = Mesh(mesh.devices.reshape(8, 4, 4, 2), ALL)
    channels = P(TP, SP)
    placed = (
        P(ALL, None),
        channels,
        channels,
        channels,
        channels,
        channels,
        channels,
        P(TP),
        P(TP, SP),
        P(TP),
        P(TP, None),
        P(),
        P(SP, TP),
        P(SP, TP),
        P(TP, SP),
    )
    return jax.shard_map(
        local, mesh=torus, in_specs=placed, out_specs=P(ALL, None), check_vma=False
    )
```

```python
import functools

import jax
import jax.numpy as jnp
from jax import lax
from jax.experimental import pallas as pl
from jax.experimental.pallas import tpu as pltpu
from jax.sharding import Mesh
from jax.sharding import PartitionSpec as P

HEAD = 64
BLOCK = 64
GROUPS = 4
SPAN = 256
BLOCKS = SPAN // BLOCK
SP = ("z", "x")
TP = ("y", "c")
ALL = ("z", "x", "y", "c")

norm_eps = 1e-06
group_eps = 0.00064
key_eps = 1e-06
half_power = 0.6065306597126334

f32 = jnp.float32
bf16 = jnp.bfloat16


def pair(a):
    if a.dtype == bf16:
        return (a,)
    high = a.astype(bf16)
    return (high, (a - high.astype(f32)).astype(bf16))


def mm(a, b, dims=((1,), (0,))):
    a = a if isinstance(a, tuple) else pair(a)
    b = b if isinstance(b, tuple) else pair(b)
    dot = lambda l, r: lax.dot_general(l, r, (dims, ((), ())), preferred_element_type=f32)
    total = dot(a[0], b[0])
    if len(b) > 1:
        total = total + dot(a[0], b[1])
    if len(a) > 1:
        total = total + dot(a[1], b[0])
    return total


def sigmoid(x):
    return 1.0 / (1.0 + jnp.exp(-x))


def down_rows(row, width):
    turned = jnp.broadcast_to(row, (128, row.shape[1])).T
    return jnp.concatenate([turned] * (width // 128), axis=1)


def head_rows(h):
    return slice(h * HEAD, (h + 1) * HEAD)


def compressed_iotas():
    row = lax.broadcasted_iota(jnp.int32, (HEAD, SPAN), 0)
    lane = lax.broadcasted_iota(jnp.int32, (HEAD, SPAN), 1)
    return row, lane % BLOCK, lane // BLOCK


def same_block():
    row = lax.broadcasted_iota(jnp.int32, (SPAN, SPAN), 0) // BLOCK
    return jnp.where(row == lax.broadcasted_iota(jnp.int32, (SPAN, SPAN), 1) // BLOCK, 1.0, 0.0)


def spread(block, every):
    return jnp.concatenate([block] * BLOCKS, axis=0) * every


def by_block(left, right, every, turned=False):
    count = left.shape[0]
    dims = (((1,), (1,)) if turned else ((1,), (0,)), ((), ()))
    dot = lambda l, r: lax.dot_general(l, spread(r, every), dims, preferred_element_type=f32)
    left, right = pair(left), pair(right)
    if len(left) == 1:
        return dot(left[0], right[0]) + dot(left[0], right[1])
    both = dot(jnp.concatenate(left, axis=0), right[0])
    return both[:count] + both[count:] + dot(left[0], right[1])


def diagonal(full, block):
    total = jnp.where(block == 0, full[:HEAD], 0.0)
    for b in range(1, BLOCKS):
        total = total + jnp.where(block == b, full[b * HEAD : (b + 1) * HEAD], 0.0)
    return total


def reached(removal, scaled, seen, block):
    left = pair(jnp.concatenate([removal.T, scaled.T], axis=0))
    seen = pair(seen)
    dot = lambda l, r: jnp.dot(l, r, preferred_element_type=f32)
    both = dot(jnp.concatenate(left, axis=0), seen[0])
    both = both[: 2 * SPAN] + both[2 * SPAN :] + dot(left[0], seen[1])
    return diagonal(both[:SPAN], block), diagonal(both[SPAN:], block)


def local_kernel(
    key_ref, value_ref, query_ref, fading_ref, rate_ref, bias_ref, surplus_ref,
    pack_ref, prefix_ref, basis_ref, removal_ref, scaled_ref, reads_ref,
):
    every = same_block()
    row = lax.broadcasted_iota(jnp.int32, (SPAN, SPAN), 0)
    col = lax.broadcasted_iota(jnp.int32, (SPAN, SPAN), 1)
    upto = jnp.where(row <= col, every, 0.0).astype(bf16)
    every = every.astype(bf16)
    fading = fading_ref[...].astype(f32) + down_rows(bias_ref[...], SPAN)
    surplus = jnp.concatenate(
        [jnp.broadcast_to(surplus_ref[h : h + 1, :], (HEAD, SPAN)) for h in range(GROUPS)], axis=0
    )
    log_decay = surplus - half_power * sigmoid(fading)
    rate = sigmoid(rate_ref[...].astype(f32))
    keys = key_ref[...].astype(f32)
    norms = jnp.concatenate(
        [
            jnp.broadcast_to(
                lax.rsqrt(
                    jnp.sum(keys[head_rows(h)] * keys[head_rows(h)], axis=0, keepdims=True) + key_eps
                ),
                (HEAD, SPAN),
            )
            for h in range(GROUPS)
        ],
        axis=0,
    )
    unit = keys * norms
    scaled = keys * rate
    removal = unit * rate
    first = log_decay.astype(bf16)
    rest = log_decay - first.astype(f32)
    second = rest.astype(bf16)
    third = (rest - second.astype(f32)).astype(bf16)
    pieces = jnp.concatenate([first, second, third], axis=0)

    def running(m):
        sums = jnp.dot(pieces, m, preferred_element_type=f32)
        return sums[:SPAN] + sums[SPAN : 2 * SPAN] + sums[2 * SPAN :]

    after = running(upto)
    final = running(every)
    probe = unit * jnp.exp(after - log_decay)
    grow = jnp.exp(-after)
    removal_in = removal * grow
    scaled_in = scaled * grow
    end = jnp.exp(final - after)
    removal_end = removal * end
    scaled_end = scaled * end
    block_decay = jnp.exp(final)
    removal_ref[...] = removal_in
    scaled_ref[...] = scaled_in
    reads_ref[...] = query_ref[...].astype(f32) * jnp.exp(after)
    row, col, block = compressed_iotas()
    eye = (row == col).astype(f32)
    strict = row < col
    in16 = (row // 16) == (col // 16)
    in32 = (row // 32) == (col // 32)
    links = ((row // 16) != (col // 16)) & in32, ~in32
    heads = range(GROUPS)
    row_of = [head_rows(h) for h in heads]
    grams = [reached(removal_in[r], scaled_in[r], probe[r], block) for r in row_of]
    mutual = [jnp.where(strict, gram[0], 0.0) for gram in grams]
    through = [jnp.where(strict, gram[1], 0.0) for gram in grams]
    values = [value_ref[r, :] for r in row_of]
    power = [jnp.where(in16, -m, 0.0) for m in mutual]
    inverse = [eye + p for p in power]
    power = [by_block(p, p, every) for p in power]
    seen = [by_block(v, t, every) for v, t in zip(values, through)]
    given = [by_block(v, scaled_end[r], every, turned=True) for v, r in zip(values, row_of)]
    for level in range(2):
        both = [
            by_block(jnp.concatenate([p, i], axis=0), p, every) for p, i in zip(power, inverse)
        ]
        power = [two[:HEAD] for two in both]
        inverse = [i + two[HEAD:] for i, two in zip(inverse, both)]
    inverse = [i + by_block(i, p, every) for i, p in zip(inverse, power)]
    for link in links:
        bridge = [by_block(i, jnp.where(link, m, 0.0), every) for i, m in zip(inverse, mutual)]
        inverse = [i - by_block(k, i, every) for i, k in zip(inverse, bridge)]
    basis = [
        by_block(jnp.concatenate([probe[r], k], axis=0), i, every)
        for r, k, i in zip(row_of, seen, inverse)
    ]
    taken = [by_block(k, removal_end[r], every, turned=True) for k, r in zip(basis, row_of)]
    carry_maps = [eye * block_decay[r] - t[:HEAD] for r, t in zip(row_of, taken)]
    carry_adds = [g - t[HEAD:] for g, t in zip(given, taken)]
    total = [
        jnp.concatenate([m[:, :HEAD], k[:, :HEAD]], axis=0) for m, k in zip(carry_maps, carry_adds)
    ]
    start = jnp.concatenate([eye[:, :HEAD], jnp.zeros((HEAD, HEAD), f32)], axis=0)
    prefix = [[start] for h in heads]
    for b in range(1, BLOCKS):
        at = slice(b * BLOCK, (b + 1) * BLOCK)
        for h in heads:
            prefix[h].append(total[h])
        total = [mm(t, m[:, at]) for t, m in zip(total, carry_maps)]
        total = [
            jnp.concatenate([t[:HEAD], t[HEAD:] + k[:, at]], axis=0) for t, k in zip(total, carry_adds)
        ]
    for h in heads:
        pack_ref[row_of[h], :] = jnp.concatenate([total[h][:HEAD], total[h][HEAD:]], axis=1).astype(bf16)
        basis_ref[h] = basis[h]
        prefix_ref[h] = jnp.concatenate(prefix[h], axis=1)


def reach_kernel(
    prefix_ref, basis_ref, removal_ref, scaled_ref, reads_ref, value_ref, state_ref, own_ref
):
    every = same_block().astype(bf16)
    row, col, block = compressed_iotas()
    upto = row <= col
    row_of = [head_rows(h) for h in range(GROUPS)]
    reads = [reads_ref[r, :] for r in row_of]
    grams = [
        reached(removal_ref[r, :], scaled_ref[r, :], q, block) for r, q in zip(row_of, reads)
    ]
    lost = [
        by_block(basis_ref[h], jnp.where(upto, gram[0], 0.0), every) for h, gram in enumerate(grams)
    ]
    own = [
        by_block(value_ref[r, :], jnp.where(upto, gram[1], 0.0), every)
        for r, gram in zip(row_of, grams)
    ]
    both = [by_block(prefix_ref[h], reads[h] - lost[h][:HEAD], every) for h in range(GROUPS)]
    for h, r in enumerate(row_of):
        state_ref[r, :] = both[h][:HEAD]
        own_ref[r, :] = own[h] - lost[h][HEAD:] + both[h][HEAD:]


def after_pack(total, pack):
    moved = mm(total, pack[:, :HEAD])
    return jnp.concatenate(
        [moved[:HEAD], moved[HEAD:] + pack[:, HEAD:].astype(f32)], axis=0
    )


def row_kernel(index_ref, own_ref, one_ref, two_ref, three_ref, pack_ref, before_ref, held):
    mine = index_ref[1]
    for shift, ref in enumerate((own_ref, one_ref, two_ref, three_ref)):
        held[(mine + 4 - shift) % 4] = ref[...]
    eye = (
        lax.broadcasted_iota(jnp.int32, (HEAD, HEAD), 0)
        == lax.broadcasted_iota(jnp.int32, (HEAD, HEAD), 1)
    ).astype(f32)
    start = jnp.concatenate([eye, jnp.zeros((HEAD, HEAD), f32)], axis=0)
    heads = range(GROUPS)
    members = [[held[k, head_rows(h), :] for k in range(4)] for h in heads]
    first = [
        jnp.concatenate([m[0][:, :HEAD], m[0][:, HEAD:]], axis=0).astype(f32) for m in members
    ]
    second = [after_pack(f, m[1]) for f, m in zip(first, members)]
    third = [after_pack(f, m[2]) for f, m in zip(second, members)]
    fourth = [after_pack(f, m[3]) for f, m in zip(third, members)]
    for h in heads:
        before_ref[h] = jnp.where(
            mine == 0, start, jnp.where(mine == 1, first[h], jnp.where(mine == 2, second[h], third[h]))
        )
        pack_ref[head_rows(h), :] = jnp.concatenate(
            [fourth[h][:HEAD], fourth[h][HEAD:]], axis=1
        ).astype(bf16)


def window_kernel(two_ref, one_ref, own_ref, pack_ref):
    row_of = [head_rows(h) for h in range(GROUPS)]
    total = [
        jnp.concatenate([two_ref[r, :HEAD], two_ref[r, HEAD:]], axis=0) for r in row_of
    ]
    for ref in (one_ref, own_ref):
        total = [after_pack(t, ref[r, :]) for t, r in zip(total, row_of)]
    for t, r in zip(total, row_of):
        pack_ref[r, :] = jnp.concatenate([t[:HEAD], t[HEAD:]], axis=1).astype(bf16)


def mixed_kernel(
    index_ref, six_ref, three_ref, two_ref, one_ref, before_ref, state_ref, own_ref, switch_ref, scaler_ref,
    keep_ref, send_ref, held,
):
    y = index_ref[2]
    core = index_ref[3]
    carried = [six_ref[head_rows(h), HEAD:].astype(f32) for h in range(GROUPS)]
    for ref in (three_ref, two_ref, one_ref):
        for h in range(GROUPS):
            member = ref[head_rows(h), :]
            carried[h] = mm(carried[h], member[:, :HEAD]) + member[:, HEAD:].astype(f32)
    row_of = [head_rows(h) for h in range(GROUPS)]
    entering = [
        mm(carried[h], before_ref[h, :HEAD]) + before_ref[h, HEAD:] for h in range(GROUPS)
    ]
    outputs = [mm(e, state_ref[r, :]) + own_ref[r, :] for e, r in zip(entering, row_of)]
    centred = [o - jnp.mean(o, axis=0, keepdims=True) for o in outputs]
    heads = [
        k * lax.rsqrt(jnp.mean(k * k, axis=0, keepdims=True) + group_eps) for k in centred
    ]
    mixed = jnp.concatenate(heads, axis=0) * down_rows(scaler_ref[...], SPAN)
    mixed = mixed * switch_ref[...].astype(f32)
    held[...] = mixed.T.astype(bf16).reshape(8, 32, SPAN)
    for s in range(4):
        at = 2 * ((y + s) % 4)
        keep_ref[s] = held[at + core]
        send_ref[s] = held[at + 1 - core]


def project_kernel(keep_ref, got_ref, own_ref, other_ref, here_ref, one_ref, two_ref, three_ref):
    dot = functools.partial(jnp.dot, preferred_element_type=f32)
    rows = dot(keep_ref[...].reshape(128, SPAN), own_ref[...])
    rows = rows + dot(got_ref[...].reshape(128, SPAN), other_ref[...])
    here_ref[...] = rows[:32]
    one_ref[...] = rows[32:64].astype(bf16)
    two_ref[...] = rows[64:96].astype(bf16)
    three_ref[...] = rows[96:].astype(bf16)


VMEM = pl.BlockSpec(memory_space=pltpu.VMEM)
SMEM = pl.BlockSpec(memory_space=pltpu.SMEM)


def like(shape, kind=f32):
    return jax.ShapeDtypeStruct(shape, kind)


def whole(kernel, outs, *args, scratch=(), scalars=0, flops=0, name=None):
    specs = [SMEM] * scalars + [VMEM] * (len(args) - scalars)
    return pl.pallas_call(
        kernel,
        out_shape=outs,
        in_specs=specs,
        out_specs=jax.tree.map(lambda _: VMEM, outs),
        scratch_shapes=scratch,
        cost_estimate=pl.CostEstimate(flops=flops, transcendentals=0, bytes_accessed=1 << 20),
        name=name,
    )(*args)


def moved(x, axis, shift):
    size = lax.axis_size(axis)
    return lax.ppermute(x, axis, [(k, (k + shift) % size) for k in range(size)])


def carried_on(x, axis, shift):
    size = lax.axis_size(axis)
    return lax.ppermute(x, axis, [(k, k + shift) for k in range(size - shift)])


def rms_rows(middle, dense_block_scaler):
    scale_rows = lax.rsqrt(jnp.mean(middle * middle, axis=-1, keepdims=True) + norm_eps)
    return (middle * scale_rows * dense_block_scaler).astype(bf16)


def dense_kernel(width, index_ref, *refs):
    rows_refs = refs[:5]
    near_ref, far_ref, out_refs = refs[5], refs[6], refs[7:12]
    rows, weights, sems = refs[12:]
    half = index_ref[1] // 2
    core = index_ref[3]
    copies = []
    for z in range(8):
        copies.append([])
        for ref, parity in ((near_ref, core), (far_ref, 1 - core)):
            for k in range(2):
                to = HEAD * (4 * z + 2 * ((half + k) % 2) + parity)
                copies[-1].append(
                    pltpu.make_async_copy(
                        ref.at[pl.ds(2 * HEAD * z + HEAD * k, HEAD)],
                        weights.at[pl.ds(pl.multiple_of(to, HEAD), HEAD)],
                        sems.at[z],
                    )
                )
    for group in copies:
        for copy in group:
            copy.start()
    places = []
    for ref in rows_refs:
        at = places[-1].stop if places else 0
        places.append(slice(at, at + ref.shape[0]))
        rows[places[-1], :] = ref[...]
    sums = None
    for z in range(8):
        for copy in copies[z]:
            copy.wait()
        if z % 2 == 0:
            continue
        at = slice((z - 1) * SPAN, (z + 1) * SPAN)
        part = jnp.dot(rows[:, at], weights[at, : 2 * width], preferred_element_type=f32)
        sums = part if sums is None else sums + part
    gate_sum = sums[:, :width]
    hidden = (gate_sum * sigmoid(gate_sum) * sums[:, width:]).astype(bf16)
    out = lax.dot_general(
        hidden, weights[:, 2 * width : 3 * width], (((1,), (1,)), ((), ())), preferred_element_type=f32
    ).astype(bf16)
    for place, ref in zip(places, out_refs):
        ref[...] = out[place]


def across(x):
    return lax.ppermute(x, "x", [(k, k ^ 1) for k in range(4)])


def to_parity(x, flip):
    pairs = []
    for place in range(4):
        for core in range(2):
            chip = core + 2 * ((place // 2) ^ flip)
            pairs.append((2 * place + core, 2 * chip + place % 2))
    return lax.ppermute(x, ("x", "c"), pairs)


def local(
    residual_matrix,
    query_vectors,
    lookup_vectors,
    payload_vectors,
    fading_dependent_term,
    step_size_preactivation,
    attention_result_switch,
    fading_bias_vector,
    surplus_forgetting,
    per_group_scaler,
    attention_result_matrix,
    dense_block_scaler,
    switching_matrix,
    expanding_matrix,
    contracting_matrix,
):
    index = jnp.stack([lax.axis_index(a) for a in ALL]).astype(jnp.int32)
    hidden_width = switching_matrix.shape[1]
    blank = jnp.zeros((switching_matrix.shape[0], -3 * hidden_width % 128), bf16)
    shard = jnp.concatenate(
        [switching_matrix, expanding_matrix, contracting_matrix.T, blank], axis=1
    )
    arriving = (to_parity(shard, 0), to_parity(shard, 1))
    other_matrix = moved(attention_result_matrix, "c", 1)
    full = like((SPAN, SPAN))
    wide = like((GROUPS, 2 * HEAD, SPAN))
    pack, *parts = whole(
        local_kernel,
        (like((SPAN, 128), bf16), wide, wide, full, full, full),
        lookup_vectors,
        payload_vectors,
        query_vectors,
        fading_dependent_term,
        step_size_preactivation,
        fading_bias_vector.reshape(1, -1),
        surplus_forgetting,
        flops=1 << 33,
        name="local",
    )
    *arrived, _ = lax.optimization_barrier((*arriving, pack))
    near = lax.all_gather(jnp.concatenate(arrived, axis=0), "z", axis=0, tiled=True)
    others = [moved(pack, "x", s) for s in (1, 2, 3)]
    state, own = whole(
        reach_kernel, (full, full), *parts, payload_vectors, flops=1 << 32, name="reach",
    )
    row_pack, before = whole(
        row_kernel,
        (like((SPAN, 128), bf16), like((GROUPS, 128, HEAD))),
        index, pack, *others,
        scratch=[pltpu.VMEM((4, SPAN, 128), bf16)],
        scalars=1, flops=1 << 30, name="row",
    )
    close = [carried_on(row_pack, "z", s) for s in (2, 1)]
    window = whole(
        window_kernel, like((SPAN, 128), bf16), *close, row_pack, flops=1 << 30, name="window"
    )
    distant = [carried_on(window, "z", s) for s in (6, 3)]
    keep, send = whole(
        mixed_kernel,
        (like((4, 32, SPAN), bf16), like((4, 32, SPAN), bf16)),
        index, *distant, *close, before, state, own, attention_result_switch, per_group_scaler.reshape(1, -1),
        scratch=[pltpu.VMEM((8, 32, SPAN), bf16)],
        scalars=1, flops=1 << 30, name="mixed",
    )
    got = moved(send, "c", 1)
    here, *away = whole(
        project_kernel,
        (like((32, 2048)),) + (like((32, 2048), bf16),) * 3,
        keep, got, attention_result_matrix, other_matrix,
        flops=1 << 29, name="project",
    )
    middle = residual_matrix.astype(f32) + here
    for s, piece in enumerate(away, 1):
        middle = middle + moved(piece, "y", s).astype(f32)
    normed = rms_rows(middle, dense_block_scaler)
    both = jnp.concatenate([normed, across(normed)], axis=0)
    own_half, _ = lax.optimization_barrier((near, both))
    far = moved(own_half, "c", 1)
    half = normed.shape[0]
    ahead = moved(both, "y", 1)
    behind = moved(both, "y", -1)
    rows = [both, ahead, behind, moved(ahead[:half], "y", 1), moved(behind[half:], "y", -1)]
    width = normed.shape[1]
    parts = pl.pallas_call(
        functools.partial(dense_kernel, hidden_width),
        out_shape=tuple(like(part.shape, bf16) for part in rows),
        in_specs=[SMEM] + [VMEM] * 5 + [pl.BlockSpec(memory_space=pl.ANY), VMEM],
        out_specs=(VMEM,) * 5,
        scratch_shapes=[
            pltpu.VMEM((SPAN, width), bf16),
            pltpu.VMEM((width, near.shape[1]), bf16),
            pltpu.SemaphoreType.DMA((8,)),
        ],
        compiler_params=pltpu.CompilerParams(vmem_limit_bytes=40 << 20),
        name="dense",
    )(index, *rows, near, far)
    own, low, high, low_half, high_half = [part.astype(f32) for part in parts]
    below = moved(parts[3], "y", -1).astype(f32)
    above = moved(parts[4], "y", 1).astype(f32)
    low = jnp.concatenate([low[:half] + below, low[half:]], axis=0).astype(bf16)
    high = jnp.concatenate([high[:half], high[half:] + above], axis=0).astype(bf16)
    pair_out = own + moved(low, "y", -1).astype(f32) + moved(high, "y", 1).astype(f32)
    channel_out = pair_out[:32] + across(pair_out[32:].astype(bf16)).astype(f32)
    return (middle + channel_out).astype(bf16)


def solution(mesh):
    torus = Mesh(mesh.devices.reshape(8, 4, 4, 2), ALL)
    channels = P(TP, SP)
    placed = (
        P(ALL, None),
        channels,
        channels,
        channels,
        channels,
        channels,
        channels,
        P(TP),
        P(TP, SP),
        P(TP),
        P(TP, None),
        P(),
        P(SP, TP),
        P(SP, TP),
        P(TP, SP),
    )
    return jax.shard_map(
        local, mesh=torus, in_specs=placed, out_specs=P(ALL, None), check_vma=False
    )
```
